512 devices in a mesh: kv: 128 (over z, x, core), tp: 4 (over y).
Axes of the slice: x: 4, y: 4, z: 16, core: 2. Of those that a mesh axis runs over, the one named last changes fastest.
Arguments:
- queries: bfloat16 [16384, 4096], P('kv', 'tp'), may hold values from -6 to 6
- keys: bfloat16 [16384, 512], P('kv', 'tp'), may hold values from -6 to 6
- values: bfloat16 [16384, 512], P('kv', 'tp'), may hold values from -6 to 6
- logsum: float32 [16384, 32], P('kv', 'tp'), may hold values from 2 to 6
- out_grad: bfloat16 [16384, 4096], P('kv', 'tp'), may hold values from -6 to 6
- normed_input: bfloat16 [16384, 4096], P('kv', 'tp'), may hold values from -6 to 6
- chosen: int32 [256, 16], P('kv'), may hold values from 0 to 511, as said below
Outputs:
- query_grad: float32 [16384, 4096], P('kv', 'tp')
- key_grad: float32 [16384, 512], P('kv', 'tp')
- value_grad: float32 [16384, 512], P('kv', 'tp')
- value_weight_grad: float32 [4096, 512], P('kv', 'tp')
The draws below stay inside these ranges and needn't reach their ends.
Inputs may be any that keep to these rules, and one draw needn't show every extreme that they name: `chosen`: each row r names 16 distinct key blocks, among them block 0 and the blocks r * 2 to r * 2 + 64 / 32 - 1 that hold the query block's own positions. The rows of one device (aligned runs of 2 rows) name at most one block of any other device's 128 / 32 blocks. Blocks after the query block may be named; their keys are masked.
All inputs are finite; a program needn't handle non-finite values.
Results may differ from the reference program's by a relative error of at most 0.008.
Values may be sent and summed in bfloat16 or wider, within the bound.
No kernel may reach another device: no remote copies, remote signals or barrier semaphores. Data moves between devices by JAX's collectives and lax.ppermute only.
A program may use at most 64 MiB of HBM per device.

```python
import jax
import jax.numpy as jnp
from jax import lax

D = 4096
HEADS = 32
KV_HEADS = 4
HD = 128
TOK_DEV = 128
QB = 64
KB = 32
NSEL = 16
TOKENS = 16384


def draw_chosen(key, part):
    kblock_count = TOK_DEV // KB
    qblock_count = TOK_DEV // QB
    devices = TOKENS // TOK_DEV
    row_count = TOKENS // QB
    diag = QB // KB
    ncand = devices + kblock_count
    key_pick = jax.random.fold_in(key, 11)
    key_pop = jax.random.fold_in(key, 12)
    key_far = jax.random.fold_in(key, 13)
    key_own = jax.random.fold_in(key, 14)
    owners = jnp.arange(devices, dtype=jnp.int32)
    pick = jax.random.randint(key_pick, (devices, devices), 0, kblock_count)
    pick = jnp.where(owners[None, :] == 0, 0, pick)
    popular = jax.random.randint(key_pop, (devices,), 0, 8)
    rows = jnp.arange(row_count, dtype=jnp.int32)
    device_of = rows // qblock_count
    first = rows * diag
    remote_blk = owners[None, :] * kblock_count + pick[device_of]
    own_blk = device_of[:, None] * kblock_count + jnp.arange(kblock_count, dtype=jnp.int32)[None, :]
    cand = jnp.concatenate([remote_blk, own_blk], axis=1)
    cand_owner = cand // kblock_count
    slot_owner = jnp.concatenate([owners, jnp.full((kblock_count,), -1, jnp.int32)])
    is_diag = (cand >= first[:, None]) & (cand < first[:, None] + diag)
    invalid = (slot_owner[None, :] == device_of[:, None]) | is_diag
    forced = (cand == 0) | (cand_owner == device_of[:, None] - 1) | (cand_owner == device_of[:, None] - devices // 2)
    causal = cand < first[:, None]
    far_noise = jax.random.randint(key_far, (row_count, devices), 0, 32) + popular[None, :]
    own_noise = jax.random.randint(key_own, (row_count, kblock_count), 0, 32)
    noise = jnp.concatenate([far_noise, own_noise], axis=1)
    tier = jnp.where(forced, 3, jnp.where(causal, 2, 1))
    index = jnp.arange(ncand, dtype=jnp.int32)[None, :]
    score = jnp.where(invalid, 0, tier * 64 + noise) * ncand + (ncand - 1 - index)
    _, top = lax.top_k(score, NSEL - diag)
    picked = jnp.take_along_axis(cand, top, axis=1)
    diag_ids = first[:, None] + jnp.arange(diag, dtype=jnp.int32)[None, :]
    return jnp.concatenate([diag_ids, picked], axis=1).astype(jnp.int32)


def block_levels(stream_key, extent, split, least, high):
    loudness, own = 1.0, jax.random.fold_in(stream_key, 6)
    for position, blocks in split:
        steps = jnp.exp(jax.random.uniform(jax.random.fold_in(own, position), (blocks,), jnp.float32, least / len(split), high / len(split)))
        loudness = loudness * jnp.repeat(steps, extent[position] // blocks).reshape([-1 if axis == position else 1 for axis in range(len(extent))])
    return loudness


def bell_draw(stream_key, dims, width, limit, shards=(), kind=jnp.bfloat16):
    gain = block_levels(stream_key, dims, shards, -0.22, 0.18) if shards else 1.0
    drawn = jax.random.normal(stream_key, dims, jnp.float32) * width * gain
    return jnp.minimum(jnp.maximum(drawn, -limit), limit).astype(kind)


def setup_inputs(seed: int = 0) -> dict:
    streams_of = jax.random.split(jax.random.key(seed), 8)
    return {
        "queries": bell_draw(streams_of[0], (TOKENS, HEADS * HD), 1.0, 6.0, ((0, 128), (1, 4))),
        "keys": bell_draw(streams_of[1], (TOKENS, KV_HEADS * HD), 1.0, 6.0, ((0, 128), (1, 4))),
        "values": bell_draw(streams_of[2], (TOKENS, KV_HEADS * HD), 1.0, 6.0, ((0, 128), (1, 4))),
        "logsum": jnp.clip(2.0 + 4.0 * jax.random.uniform(streams_of[3], (TOKENS, HEADS), jnp.float32) ** block_levels(streams_of[3], (TOKENS, HEADS), ((0, 128), (1, 4)), -0.2, 0.2), 2.0, 6.0),
        "out_grad": bell_draw(streams_of[4], (TOKENS, HEADS * HD), 1.0, 6.0, ((0, 128), (1, 4))),
        "normed_input": bell_draw(streams_of[5], (TOKENS, D), 1.0, 6.0, ((0, 128), (1, 4))),
        "chosen": draw_chosen(jax.random.fold_in(streams_of[7], 71), 0),
    }


def reference(queries, keys, values, logsum, out_grad, normed_input, chosen):
    group = HEADS // KV_HEADS
    kv_cols = KV_HEADS * HD
    scale = HD ** -0.5
    blocks = TOKENS // KB
    key_blocks = keys.reshape(blocks, KB, KV_HEADS, HD)
    value_blocks = values.reshape(blocks, KB, KV_HEADS, HD)
    offsets = jnp.arange(KB, dtype=jnp.int32)
    rows_in = jnp.arange(QB, dtype=jnp.int32)

    def step(carry, index):
        key_acc, value_acc = carry
        ids = chosen[index]
        start = index * QB
        query_rows = lax.dynamic_slice_in_dim(queries, start, QB, 0).reshape(QB, KV_HEADS, group, HD).astype(jnp.float32)
        dout = lax.dynamic_slice_in_dim(out_grad, start, QB, 0).reshape(QB, KV_HEADS, group, HD).astype(jnp.float32)
        lse = lax.dynamic_slice_in_dim(logsum, start, QB, 0).reshape(QB, KV_HEADS, group)
        sel_keys = key_blocks[ids].reshape(NSEL * KB, KV_HEADS, HD).astype(jnp.float32)
        sel_values = value_blocks[ids].reshape(NSEL * KB, KV_HEADS, HD).astype(jnp.float32)
        scores = jnp.einsum("qngd,jnd->qngj", query_rows, sel_keys) * scale
        qpos = start + rows_in
        kpos = (ids[:, None] * KB + offsets[None, :]).reshape(NSEL * KB)
        valid = (kpos[None, :] <= qpos[:, None])[:, None, None, :]
        prob = jnp.where(valid, jnp.exp(scores - lse[..., None]), 0.0)
        dprob = jnp.einsum("qngd,jnd->qngj", dout, sel_values)
        delta = jnp.sum(prob * dprob, axis=-1, keepdims=True)
        dscore = lax.optimization_barrier((prob * (dprob - delta)).astype(jnp.bfloat16)).astype(jnp.float32)
        prob_low = lax.optimization_barrier(prob.astype(jnp.bfloat16)).astype(jnp.float32)
        query_part = jnp.einsum("qngj,jnd->qngd", dscore, sel_keys) * scale
        key_part = jnp.einsum("qngj,qngd->jnd", dscore, query_rows) * scale
        value_part = jnp.einsum("qngj,qngd->jnd", prob_low, dout)
        key_acc = key_acc.at[ids].add(key_part.reshape(NSEL, KB * kv_cols))
        value_acc = value_acc.at[ids].add(value_part.reshape(NSEL, KB * kv_cols))
        return (key_acc, value_acc), query_part.reshape(QB, HEADS * HD)

    zeros = jnp.zeros((blocks, KB * kv_cols), jnp.float32)
    (key_acc, value_acc), query_rows_all = lax.scan(step, (zeros, zeros), jnp.arange(TOKENS // QB, dtype=jnp.int32))
    query_grad = query_rows_all.reshape(TOKENS, HEADS * HD)
    key_grad = key_acc.reshape(TOKENS, kv_cols)
    value_grad = value_acc.reshape(TOKENS, kv_cols)
    value_low = value_grad.astype(jnp.bfloat16)
    weight_grad = jnp.dot(normed_input.astype(jnp.float32).T, value_low.astype(jnp.float32))
    return query_grad, key_grad, value_grad, weight_grad
```

```python
import jax
import jax.numpy as jnp
from jax import lax
from jax.sharding import Mesh
from jax.sharding import PartitionSpec as P

HD = 128
QB = 64
KB = 32
NSEL = 16
KV = ("z", "x", "c")
XC = ("x", "c")


def to_peers(parts, axis):
    return lax.all_to_all(parts, axis, split_axis=0, concat_axis=0, tiled=True)


def local(queries, keys, values, logsum, out_grad, normed_input, chosen):
    nz = lax.axis_size("z")
    nq = lax.axis_size(XC)
    tp = lax.axis_size("tp")
    here = lax.axis_index(KV)
    tok = keys.shape[0]
    kblocks = tok // KB
    qblocks = tok // QB
    group = queries.shape[1] // HD
    span = NSEL * KB
    scale = HD ** (-0.5)
    peers = nq * nz
    entries = qblocks * NSEL

    owner = chosen // kblocks
    within = chosen % kblocks
    remote = owner != here
    place = (owner % nq) * nz + owner // nq
    named = (place[:, :, None] == jnp.arange(peers, dtype=jnp.int32)) & remote[:, :, None]
    wanted = jnp.max(jnp.where(named, within[:, :, None] + 1, 0), axis=(0, 1))
    asked = to_peers(wanted.reshape(nq, nz), XC)
    slot = jnp.where(remote, place, peers + within).reshape(entries)
    taken = jnp.arange(nz, dtype=jnp.int32)[None, :] * kblocks + jnp.maximum(asked - 1, 0)

    def fetch(rows):
        column = lax.all_gather(rows, "z", axis=0, tiled=True).reshape(nz * kblocks, KB, HD)
        got = to_peers(column[taken.reshape(-1)].reshape(nq, nz * KB, HD), XC)
        pool = jnp.concatenate([got.reshape(peers, KB, HD), rows.reshape(kblocks, KB, HD)], axis=0)
        return pool[slot].reshape(qblocks, span, HD)

    onehot = (slot[:, None] == jnp.arange(peers + kblocks, dtype=jnp.int32)[None, :]).astype(jnp.float32)
    home = ((asked - 1)[:, :, None] == jnp.arange(kblocks, dtype=jnp.int32)).astype(jnp.bfloat16)

    def give_back(part):
        total = jnp.dot(
            onehot.T,
            part.reshape(entries, KB * HD),
            precision=lax.Precision.HIGHEST,
            preferred_element_type=jnp.float32,
        )
        own = total[peers:].reshape(tok, HD)
        sent = total[:peers].astype(jnp.bfloat16).reshape(nq, nz * KB, HD)
        came = to_peers(sent, XC).reshape(nq, nz, KB * HD)
        dense = jnp.einsum("qzk,qze->zke", home, came, preferred_element_type=jnp.float32)
        dense = dense.astype(jnp.bfloat16).reshape(nz, tok, HD)
        sums = to_peers(dense, "z")
        return own + jnp.sum(sums.astype(jnp.float32), axis=0)

    feats = normed_input.shape[1]
    rows_out = feats * tp // peers
    mine = nz // tp
    split = normed_input.reshape(tok, mine, nq, rows_out).transpose(2, 0, 1, 3)
    split = to_peers(split.reshape(nq, tok, mine * rows_out), XC).reshape(nq * tok, mine * rows_out)
    planes = [split]
    for k in range(1, tp):
        planes.append(lax.ppermute(split, "tp", [(i, (i + k) % tp) for i in range(tp)]))

    sel_keys = fetch(keys)
    query_rows = queries.reshape(qblocks, QB, group, HD)
    dout = out_grad.reshape(qblocks, QB, group, HD)
    lse = logsum.reshape(qblocks, QB, group)
    scores = (
        jnp.einsum("bqgd,bjd->bqgj", query_rows, sel_keys, preferred_element_type=jnp.float32)
        * scale
    )
    qpos = here * tok + jnp.arange(tok, dtype=jnp.int32).reshape(qblocks, QB)
    kpos = (chosen[:, :, None] * KB + jnp.arange(KB, dtype=jnp.int32)[None, None, :]).reshape(
        qblocks, span
    )
    valid = (kpos[:, None, :] <= qpos[:, :, None])[:, :, None, :]
    prob = jnp.where(valid, jnp.exp(scores - lse[..., None]), 0.0)
    prob_low = prob.astype(jnp.bfloat16)
    value_grad = give_back(
        jnp.einsum("bqgj,bqgd->bjd", prob_low, dout, preferred_element_type=jnp.float32)
    )

    value_low = value_grad.astype(jnp.bfloat16)
    all_low = lax.all_gather(value_low, XC, axis=0, tiled=True)
    me = lax.axis_index("tp")
    products = jnp.stack(
        [jnp.einsum("tf,tc->fc", p, all_low, preferred_element_type=jnp.float32) for p in planes]
    )
    order = (me - jnp.arange(tp)) % tp
    products = products[order].astype(jnp.bfloat16)
    weight_parts = to_peers(products.reshape(nz, rows_out, HD), "z")
    weight_grad = jnp.sum(weight_parts.astype(jnp.float32), axis=0)

    sel_values = fetch(values)
    dprob = jnp.einsum("bqgd,bjd->bqgj", dout, sel_values, preferred_element_type=jnp.float32)
    delta = jnp.sum(prob * dprob, axis=-1, keepdims=True)
    dscore = (prob * (dprob - delta)).astype(jnp.bfloat16)
    key_grad = give_back(
        jnp.einsum("bqgj,bqgd->bjd", dscore, query_rows, preferred_element_type=jnp.float32) * scale
    )
    query_grad = (
        jnp.einsum("bqgj,bjd->bqgd", dscore, sel_keys, preferred_element_type=jnp.float32) * scale
    )
    return (query_grad.reshape(tok, group * HD), key_grad, value_grad, weight_grad)


def solution(mesh):
    kv, tp = mesh.shape["kv"], mesh.shape["tp"]
    split = Mesh(mesh.devices.reshape(kv // 8, 4, 2, tp), ("z", "x", "c", "tp"))
    cut = P(KV, "tp")
    return jax.shard_map(
        local,
        mesh=split,
        in_specs=(cut, cut, cut, cut, cut, cut, P(KV, None)),
        out_specs=(cut, cut, cut, cut),
        check_vma=False,
    )
```

```python
import functools

import jax
import jax.numpy as jnp
from jax import lax
from jax.experimental import pallas as pl
from jax.experimental.pallas import tpu as pltpu
from jax.sharding import Mesh
from jax.sharding import PartitionSpec as P

HD = 128
QB = 64
KB = 32
NSEL = 16
KV = ("z", "x", "c")
XC = ("x", "c")
SUB = 8
SCALE = HD ** (-0.5)
F32 = jnp.float32
BF16 = jnp.bfloat16
NT = (((1,), (1,)), ((), ()))
TN = (((0,), (0,)), ((), ()))


def to_peers(parts, axis):
    return lax.all_to_all(parts, axis, split_axis=0, concat_axis=0, tiled=True)


def smem():
    return pl.BlockSpec(memory_space=pltpu.SMEM)


def vmem():
    return pl.BlockSpec(memory_space=pltpu.VMEM)


def call(body, outs, ins, scratch=()):
    return pl.pallas_call(
        body,
        out_shape=outs,
        in_specs=[smem() if i == "s" else vmem() for i in ins],
        out_specs=jax.tree.map(lambda _: vmem(), outs),
        scratch_shapes=list(scratch),
        compiler_params=pltpu.CompilerParams(vmem_limit_bytes=40 * 1024 * 1024),
    )


def pick(nq, nz, asked, column, out):
    per = column.shape[0] // nz
    for q in range(nq):
        for z in range(nz):
            block = jnp.maximum(asked[q * nz + z] - 1, 0)
            out[q * nz + z] = column[z * per + block]


def by_feature(nq, rows, features, wanted, out):
    tok, cols = features.shape
    for i in range(cols // HD):
        tile = features[:, i * HD : (i + 1) * HD].T
        for j in range(HD // rows):
            piece = i * (HD // rows) + j
            out[piece % nq, (piece // nq) * rows : (piece // nq + 1) * rows] = tile[
                j * rows : (j + 1) * rows
            ]
    for q in range(nq):
        out[q, cols // nq :] = jnp.broadcast_to(wanted[q : q + 1], (SUB, tok))


def slots_of(chosen, here, b, nq, nz, kblocks):
    slots = []
    for e in range(NSEL):
        c = chosen[b * NSEL + e]
        owner = c // kblocks
        place = (owner % nq) * nz + owner // nq
        slots.append((c, owner != here, place, c % kblocks))
    return slots


def select(slots, got, own, out):
    for e, (_, remote, place, within) in enumerate(slots):
        far = got[jnp.where(remote, place, 0)]
        near = own[within]
        out[e * KB : (e + 1) * KB] = jnp.where(remote, far, near)


def heads_of(ref, b, p):
    rows = slice(b * QB, (b + 1) * QB)
    return jnp.concatenate(
        [ref[rows, (2 * p + i) * HD : (2 * p + i + 1) * HD] for i in range(2)], axis=0
    )


def set_positions(slots, kpos):
    rows = lax.broadcasted_iota(jnp.int32, (KB, HD), 0)
    lanes = lax.broadcasted_iota(jnp.int32, (KB, HD), 1) % QB
    for e, (c, _, _, _) in enumerate(slots):
        kpos[e * KB : (e + 1) * KB] = c * KB + rows - lanes


def prob_of(sel, pair, lse, kpos, start, b, p, pairs):
    scores = lax.dot_general(sel[...], pair, NT, preferred_element_type=F32) * SCALE
    at = b * pairs + p
    return jnp.where(kpos[...] <= start, jnp.exp(scores - lse[at : at + 1, :]), 0.0)


def scatter(slots, parts, total, send, own_sum, peers, kblocks):
    def put(slot):
        _, remote, place, within = slot
        return jnp.where(remote, place, peers + within)

    zero = jnp.zeros((KB, HD), F32)
    for k in range(kblocks):
        total[peers + k] = zero
    for slot in slots[1]:
        total[put(slot)] = zero
    for b, part in enumerate(parts):
        for e, slot in enumerate(slots[b]):
            piece = part[e * KB : (e + 1) * KB]
            at = put(slot)
            total[at] = total[at] + piece if b else piece
    for b in range(len(parts)):
        for _, remote, place, _ in slots[b]:

            @pl.when(remote)
            def _(place=place):
                send[place] = total[place].astype(BF16)

    for k in range(kblocks):
        own_sum[k] = total[peers + k]


def value_terms(nq, nz, chosen, here, queries, dout, lse, got_k, own_k, send, own_sum, sel, kpos, low, rows, total, part):
    peers, kblocks = nq * nz, own_k.shape[0]
    qblocks, pairs = queries.shape[0] // QB, queries.shape[1] // HD // 2
    slots = [slots_of(chosen, here[0], b, nq, nz, kblocks) for b in range(qblocks)]
    for b in range(qblocks):
        select(slots[b], got_k, own_k, sel)
        set_positions(slots[b], kpos)
        start = here[0] * queries.shape[0] + b * QB
        for p in range(pairs):
            pair = heads_of(queries, b, p)
            prob = prob_of(sel, pair, lse, kpos, start, b, p, pairs)
            low[:, p * HD : (p + 1) * HD] = prob.astype(BF16)
            rows[p * HD : (p + 1) * HD] = heads_of(dout, b, p)
        part[b] = jnp.dot(low[...], rows[...], preferred_element_type=F32)
    scatter(slots, [part.at[b] for b in range(qblocks)], total, send, own_sum, peers, kblocks)


def key_terms(nq, nz, chosen, here, queries, dout, lse, got_k, own_k, got_v, own_v, send, own_sum, low, sel, sel_v, kpos, rows, total, part):
    peers, kblocks = nq * nz, own_k.shape[0]
    qblocks, pairs = queries.shape[0] // QB, queries.shape[1] // HD // 2
    slots = [slots_of(chosen, here[0], b, nq, nz, kblocks) for b in range(qblocks)]
    for b in range(qblocks):
        select(slots[b], got_k, own_k, sel.at[b])
        select(slots[b], got_v, own_v, sel_v)
        set_positions(slots[b], kpos)
        start = here[0] * queries.shape[0] + b * QB
        for p in range(pairs):
            pair = heads_of(queries, b, p)
            prob = prob_of(sel.at[b], pair, lse, kpos, start, b, p, pairs)
            dprob = lax.dot_general(sel_v[...], heads_of(dout, b, p), NT, preferred_element_type=F32)
            delta = jnp.sum(prob * dprob, axis=0, keepdims=True)
            low[b, :, p * HD : (p + 1) * HD] = (prob * (dprob - delta)).astype(BF16)
            rows[p * HD : (p + 1) * HD] = pair
        part[b] = jnp.dot(low[b], rows[...], preferred_element_type=F32) * SCALE
    scatter(slots, [part.at[b] for b in range(qblocks)], total, send, own_sum, peers, kblocks)


def query_terms(low, sel, out):
    for b in range(low.shape[0]):
        for p in range(low.shape[2] // HD):
            got = lax.dot_general(
                low[b, :, p * HD : (p + 1) * HD], sel[b], TN, preferred_element_type=F32
            )
            for i in range(2):
                out[b * QB : (b + 1) * QB, (2 * p + i) * HD : (2 * p + i + 1) * HD] = (
                    got[i * QB : (i + 1) * QB] * SCALE
                )


def gather_home(nq, nz, asked, came, dense, total):
    blocks = dense.shape[0]
    kblocks = blocks // nz
    total[...] = jnp.zeros_like(total)
    for q in range(nq):
        for z in range(nz):
            a = asked[q * nz + z]
            at = jnp.where(a > 0, z * kblocks + a - 1, blocks)
            total[at] = total[at] + came[q * nz + z].astype(F32)
    dense[...] = total[0:blocks].astype(BF16)


def weight_terms(rows_out, low, dense, *refs):
    *features, order, out = refs
    nq, nz, tok = low.shape[0], dense.shape[0], dense.shape[1]
    mine = nz // len(features)
    feats = mine * rows_out
    for k, block in enumerate(features):
        total = jnp.dot(block[0, 0:feats], low[0], preferred_element_type=F32)
        for q in range(1, nq):
            total = total + jnp.dot(block[q, 0:feats], low[q], preferred_element_type=F32)
        total = total.astype(BF16)
        for a in range(mine):
            out[order[k] * mine + a, tok:] = total[a * rows_out : (a + 1) * rows_out]
    out[:, 0:tok] = dense[...]


def local(queries, keys, values, logsum, out_grad, normed_input, chosen):
    nz = lax.axis_size("z")
    nq = lax.axis_size(XC)
    tp = lax.axis_size("tp")
    here = lax.axis_index(KV)
    tok, cols = queries.shape
    kblocks = tok // KB
    qblocks = tok // QB
    heads = cols // HD
    span = NSEL * KB
    peers = nq * nz
    shape = jax.ShapeDtypeStruct

    owner = chosen // kblocks
    place = (owner % nq) * nz + owner // nq
    named = (place[:, :, None] == jnp.arange(peers, dtype=jnp.int32)) & (owner != here)[:, :, None]
    wanted = jnp.max(jnp.where(named, (chosen % kblocks)[:, :, None] + 1, 0), axis=(0, 1))
    wanted = jnp.pad(wanted.reshape(nq, nz).astype(BF16), ((0, 0), (0, tok - nz)))

    rows_out = normed_input.shape[1] * tp // peers
    mine = nz // tp
    feats = mine * rows_out
    split = call(
        functools.partial(by_feature, nq, rows_out), shape((nq, feats + SUB, tok), BF16), "vv"
    )(normed_input, wanted)
    split = to_peers(split, XC)
    asked = split[:, feats, :nz].astype(jnp.int32).reshape(peers)
    planes = [split]
    for k in range(1, tp):
        planes.append(lax.ppermute(planes[0], "tp", [(i, (i + k) % tp) for i in range(tp)]))
    order = ((lax.axis_index("tp") - jnp.arange(tp)) % tp).astype(jnp.int32)
    names = chosen.reshape(qblocks * NSEL)
    me = here.reshape(1).astype(jnp.int32)

    def fetch(rows):
        column = lax.all_gather(rows, "z", axis=0, tiled=True).reshape(nz * kblocks, KB, HD)
        sent = call(functools.partial(pick, nq, nz), shape((peers, KB, HD), BF16), "sv")(
            asked, column
        )
        return to_peers(sent.reshape(nq, nz * KB, HD), XC).reshape(peers, KB, HD)

    got_k = fetch(keys)
    got_v = fetch(values)

    own_k = keys.reshape(kblocks, KB, HD)
    own_v = values.reshape(kblocks, KB, HD)
    lse = logsum.reshape(qblocks, QB, heads).transpose(0, 2, 1).reshape(qblocks * heads // 2, 2 * QB)
    terms = (shape((peers, KB, HD), BF16), shape((kblocks, KB, HD), F32))
    work = [
        pltpu.VMEM((span, HD), jnp.int32),
        pltpu.VMEM((heads * QB, HD), BF16),
        pltpu.VMEM((peers + kblocks, KB, HD), F32),
        pltpu.VMEM((qblocks, span, HD), F32),
    ]

    def home(sent):
        came = to_peers(sent.reshape(nq, nz * KB, HD), XC).reshape(peers, KB, HD)
        dense = call(
            functools.partial(gather_home, nq, nz),
            shape((nz * kblocks, KB, HD), BF16),
            "sv",
            [pltpu.VMEM((nz * kblocks + 1, KB, HD), F32)],
        )(asked, came)
        return dense.reshape(nz, tok, HD)

    sent_v, mine_v = call(
        functools.partial(value_terms, nq, nz),
        terms,
        "ssvvvvv",
        [pltpu.VMEM((span, HD), BF16), work[0], pltpu.VMEM((span, heads * QB), BF16), *work[1:]],
    )(names, me, queries, out_grad, lse, got_k, own_k)
    dense_v = home(sent_v)
    sums_v = to_peers(dense_v, "z")
    value_grad = mine_v.reshape(tok, HD) + jnp.sum(sums_v.astype(F32), axis=0)

    sent_k, mine_k, low, sel = call(
        functools.partial(key_terms, nq, nz),
        (*terms, shape((qblocks, span, heads * QB), BF16), shape((qblocks, span, HD), BF16)),
        "ssvvvvvvv",
        [pltpu.VMEM((span, HD), BF16), *work],
    )(names, me, queries, out_grad, lse, got_k, own_k, got_v, own_v)
    dense_k = home(sent_k)
    query_grad = call(query_terms, shape((tok, cols), F32), "vv")(low, sel)

    all_low = lax.all_gather(value_grad.astype(BF16), XC, axis=0)
    both = call(
        functools.partial(weight_terms, rows_out),
        shape((nz, tok + rows_out, HD), BF16),
        "v" * (2 + tp) + "s",
    )(all_low, dense_k, *planes, order)
    both = jnp.sum(to_peers(both, "z").astype(F32), axis=0)
    key_grad = mine_k.reshape(tok, HD) + both[:tok]
    return (query_grad, key_grad, value_grad, both[tok:])


def solution(mesh):
    kv, tp = mesh.shape["kv"], mesh.shape["tp"]
    split = Mesh(mesh.devices.reshape(kv // 8, 4, 2, tp), ("z", "x", "c", "tp"))
    cut = P(KV, "tp")

    return jax.shard_map(
        local,
        mesh=split,
        in_specs=(cut, cut, cut, cut, cut, cut, P(KV, None)),
        out_specs=(cut, cut, cut, cut),
        check_vma=False,
    )
```

```python
import functools

import jax
import jax.numpy as jnp
from jax import lax
from jax.experimental import pallas as pl
from jax.experimental.pallas import tpu as pltpu
from jax.sharding import Mesh
from jax.sharding import PartitionSpec as P

HD = 128
QB = 64
KB = 32
NSEL = 16
KV = ("z", "x", "c")
XC = ("x", "c")
SUB = 8
SCALE = HD ** (-0.5)
F32 = jnp.float32
BF16 = jnp.bfloat16
NT = (((1,), (1,)), ((), ()))
TN = (((0,), (0,)), ((), ()))


def to_peers(parts, axis):
    return lax.all_to_all(parts, axis, split_axis=0, concat_axis=0, tiled=True)


def smem():
    return pl.BlockSpec(memory_space=pltpu.SMEM)


def vmem():
    return pl.BlockSpec(memory_space=pltpu.VMEM)


def call(body, outs, ins, scratch=()):
    return pl.pallas_call(
        body,
        out_shape=outs,
        in_specs=[smem() if i == "s" else vmem() for i in ins],
        out_specs=jax.tree.map(lambda _: vmem(), outs),
        scratch_shapes=list(scratch),
        compiler_params=pltpu.CompilerParams(vmem_limit_bytes=40 * 1024 * 1024),
    )


def pick(nq, nz, asked, column, out):
    per = column.shape[0] // nz
    for q in range(nq):
        for z in range(nz):
            block = jnp.maximum(asked[q * nz + z] - 1, 0)
            out[q * nz + z] = column[z * per + block]


def pick_apart(nz, asked, peer, column, *outs):
    kblocks = column.shape[0] // nz
    for d, out in enumerate(outs):
        for z in range(nz):
            block = jnp.maximum(asked[peer[d] * nz + z] - 1, 0)
            out[z] = column[z * kblocks + block]


def by_feature(nq, rows, chosen, here, features, out):
    tok, cols = features.shape
    kblocks = tok // KB
    for i in range(cols // HD):
        tile = features[:, i * HD : (i + 1) * HD].T
        for j in range(HD // rows):
            piece = i * (HD // rows) + j
            out[piece % nq, (piece // nq) * rows : (piece // nq + 1) * rows] = tile[
                j * rows : (j + 1) * rows
            ]
    at = lax.broadcasted_iota(jnp.int32, (nq, HD), 0) * HD + lax.broadcasted_iota(
        jnp.int32, (nq, HD), 1
    )
    wanted = jnp.zeros((nq, HD), F32)
    for e in range(chosen.shape[0]):
        c = chosen[e]
        owner = c // kblocks
        place = jnp.where(owner != here[0], (owner % nq) * HD + owner // nq, -1)
        wanted = jnp.where(at == place, (c % kblocks + 1).astype(F32), wanted)
    wanted = wanted.astype(BF16)
    for q in range(nq):
        out[q, cols // nq :] = jnp.broadcast_to(wanted[q : q + 1], (SUB, HD))


def slots_of(chosen, here, b, nq, nz, kblocks, where):
    slots = []
    for e in range(NSEL):
        c = chosen[b * NSEL + e]
        owner = c // kblocks
        place = where(owner % nq) * nz + owner // nq
        slots.append((c, owner != here, place, c % kblocks))
    return slots


def select(slots, got, own, out):
    for e, (_, remote, place, within) in enumerate(slots):
        near = own[within]
        if isinstance(got, tuple):
            nz = got[0].shape[0]
            d, z = place // nz, place % nz
            block = got[0][z]
            for i in range(1, len(got)):
                block = jnp.where(d == i, got[i][z], block)
        else:
            block = got[jnp.where(remote, place, 0)]
        out[e * KB : (e + 1) * KB] = jnp.where(remote, block, near)


def heads_of(ref, b, p):
    rows = slice(b * QB, (b + 1) * QB)
    return jnp.concatenate(
        [ref[rows, (2 * p + i) * HD : (2 * p + i + 1) * HD] for i in range(2)], axis=0
    )


def set_positions(slots, kpos):
    rows = lax.broadcasted_iota(jnp.int32, (KB, HD), 0)
    lanes = lax.broadcasted_iota(jnp.int32, (KB, HD), 1) % QB
    for e, (c, _, _, _) in enumerate(slots):
        kpos[e * KB : (e + 1) * KB] = c * KB + rows - lanes


def prob_of(sel, pair, lse, kpos, start, b, p, pairs):
    scores = lax.dot_general(sel[...], pair, NT, preferred_element_type=F32) * SCALE
    at = b * pairs + p
    return jnp.where(kpos[...] <= start, jnp.exp(scores - lse[at : at + 1, :]), 0.0)


def scatter(slots, parts, total, send, own_sum, peers, kblocks):
    def put(slot):
        _, remote, place, within = slot
        return jnp.where(remote, place, peers + within)

    zero = jnp.zeros((KB, HD), F32)
    for k in range(kblocks):
        total[peers + k] = zero
    for slot in slots[1]:
        total[put(slot)] = zero
    for b, part in enumerate(parts):
        for e, slot in enumerate(slots[b]):
            piece = part[e * KB : (e + 1) * KB]
            at = put(slot)
            total[at] = total[at] + piece if b else piece
    for b in range(len(parts)):
        for _, remote, place, _ in slots[b]:

            @pl.when(remote)
            def _(place=place):
                send[place] = total[place].astype(BF16)

    for k in range(kblocks):
        own_sum[k] = total[peers + k]


def value_terms(nq, nz, chosen, here, queries, dout, lse, got_k, own_k, send, own_sum, sel, kpos, low, rows, total, part):
    peers, kblocks = nq * nz, own_k.shape[0]
    qblocks, pairs = queries.shape[0] // QB, queries.shape[1] // HD // 2
    slots = [slots_of(chosen, here[0], b, nq, nz, kblocks, lambda q: q) for b in range(qblocks)]
    for b in range(qblocks):
        select(slots[b], got_k, own_k, sel)
        set_positions(slots[b], kpos)
        start = here[0] * queries.shape[0] + b * QB
        for p in range(pairs):
            pair = heads_of(queries, b, p)
            prob = prob_of(sel, pair, lse, kpos, start, b, p, pairs)
            low[:, p * HD : (p + 1) * HD] = prob.astype(BF16)
            rows[p * HD : (p + 1) * HD] = heads_of(dout, b, p)
        part[b] = jnp.dot(low[...], rows[...], preferred_element_type=F32)
    scatter(slots, [part.at[b] for b in range(qblocks)], total, send, own_sum, peers, kblocks)


def key_terms(nx, nc, nz, chosen, here, queries, dout, lse, got_k, own_k, own_v, *refs):
    nq = nx * nc
    got_v, refs = refs[:nq], refs[nq:]
    sends, refs = refs[:nq], refs[nq:]
    own_sum, low, sel, sel_v, kpos, rows, total, part, send = refs
    peers, kblocks = nq * nz, own_k.shape[0]
    qblocks, pairs = queries.shape[0] // QB, queries.shape[1] // HD // 2
    mine = here[0] % nq

    def behind(q):
        return (mine // nc - q // nc) % nx * nc + (mine + q) % nc

    def ahead(q):
        return (q // nc - mine // nc) % nx * nc + (mine + q) % nc

    def slots(b, where):
        return slots_of(chosen, here[0], b, nq, nz, kblocks, where)

    for b in range(qblocks):
        select(slots(b, lambda q: q), got_k, own_k, sel.at[b])
        select(slots(b, behind), got_v, own_v, sel_v)
        set_positions(slots(b, ahead), kpos)
        start = here[0] * queries.shape[0] + b * QB
        for p in range(pairs):
            pair = heads_of(queries, b, p)
            prob = prob_of(sel.at[b], pair, lse, kpos, start, b, p, pairs)
            dprob = lax.dot_general(sel_v[...], heads_of(dout, b, p), NT, preferred_element_type=F32)
            delta = jnp.sum(prob * dprob, axis=0, keepdims=True)
            low[b, :, p * HD : (p + 1) * HD] = (prob * (dprob - delta)).astype(BF16)
            rows[p * HD : (p + 1) * HD] = pair
        part[b] = jnp.dot(low[b], rows[...], preferred_element_type=F32) * SCALE
    back = [slots(b, ahead) for b in range(qblocks)]
    scatter(back, [part.at[b] for b in range(qblocks)], total, send, own_sum, peers, kblocks)
    for d, out in enumerate(sends):
        out[...] = send[d * nz : (d + 1) * nz]


def query_terms(low, sel, out):
    for b in range(low.shape[0]):
        for p in range(low.shape[2] // HD):
            got = lax.dot_general(
                low[b, :, p * HD : (p + 1) * HD], sel[b], TN, preferred_element_type=F32
            )
            for i in range(2):
                out[b * QB : (b + 1) * QB, (2 * p + i) * HD : (2 * p + i + 1) * HD] = (
                    got[i * QB : (i + 1) * QB] * SCALE
                )


def gather_home(nq, nz, asked, peer, *refs):
    *came, dense, total = refs
    blocks = dense.shape[0]
    kblocks = blocks // nz
    total[...] = jnp.zeros_like(total)
    for q in range(nq):
        for z in range(nz):
            a = asked[peer[q] * nz + z]
            at = jnp.where(a > 0, z * kblocks + a - 1, blocks)
            piece = came[0][q * nz + z] if len(came) == 1 else came[q][z]
            total[at] = total[at] + piece.astype(F32)
    dense[...] = total[0:blocks].astype(BF16)


def weight_terms(rows_out, low, dense, *refs):
    *features, order, out = refs
    nq, nz, tok = low.shape[0], dense.shape[0], dense.shape[1]
    mine = nz // len(features)
    feats = mine * rows_out
    for k, block in enumerate(features):
        total = jnp.dot(block[0, 0:feats], low[0], preferred_element_type=F32)
        for q in range(1, nq):
            total = total + jnp.dot(block[q, 0:feats], low[q], preferred_element_type=F32)
        total = total.astype(BF16)
        for a in range(mine):
            out[order[k] * mine + a, tok:] = total[a * rows_out : (a + 1) * rows_out]
    out[:, 0:tok] = dense[...]


def local(queries, keys, values, logsum, out_grad, normed_input, chosen):
    nz = lax.axis_size("z")
    nq = lax.axis_size(XC)
    tp = lax.axis_size("tp")
    here = lax.axis_index(KV)
    tok, cols = queries.shape
    kblocks = tok // KB
    qblocks = tok // QB
    heads = cols // HD
    span = NSEL * KB
    peers = nq * nz
    shape = jax.ShapeDtypeStruct

    names = chosen.reshape(qblocks * NSEL)
    me = here.reshape(1).astype(jnp.int32)

    rows_out = normed_input.shape[1] * tp // peers
    mine = nz // tp
    feats = mine * rows_out
    split = call(
        functools.partial(by_feature, nq, rows_out),
        shape((nq, feats + SUB, tok), BF16),
        "ssv",
    )(names, me, normed_input)
    split = to_peers(split, XC)
    asked = split[:, feats, :nz].astype(jnp.int32).reshape(peers)
    planes = [split]
    for k in range(1, tp):
        planes.append(lax.ppermute(planes[0], "tp", [(i, (i + k) % tp) for i in range(tp)]))
    order = ((lax.axis_index("tp") - jnp.arange(tp)) % tp).astype(jnp.int32)
    nx, nc = lax.axis_size("x"), lax.axis_size("c")
    steps, other = jnp.arange(nq) // nc, jnp.arange(nq) % nc
    my_x, my_c = lax.axis_index("x"), lax.axis_index("c")
    ahead = ((my_x + steps) % nx * nc + (my_c + other) % nc).astype(jnp.int32)
    behind = ((my_x - steps) % nx * nc + (my_c + other) % nc).astype(jnp.int32)
    direct = jnp.arange(nq, dtype=jnp.int32)

    def around(pieces):
        came = [pieces[0]]
        for d in range(1, nq):
            s, r = d // nc, d % nc
            pairs = [
                (x * nc + c, (x + s) % nx * nc + (c + r) % nc) for x in range(nx) for c in range(nc)
            ]
            came.append(lax.ppermute(pieces[d], XC, pairs))
        return came

    def column(rows):
        return lax.all_gather(rows, "z", axis=0, tiled=True).reshape(nz * kblocks, KB, HD)

    column_k = column(keys)
    sent = call(functools.partial(pick, nq, nz), shape((peers, KB, HD), BF16), "sv")(
        asked, column_k
    )
    got_k = to_peers(sent.reshape(nq, nz * KB, HD), XC).reshape(peers, KB, HD)
    column_v = column(values)
    slab = shape((nz, KB, HD), BF16)
    sent = call(functools.partial(pick_apart, nz), (slab,) * nq, "ssv")(asked, ahead, column_v)
    got_v = around(sent)

    own_k = keys.reshape(kblocks, KB, HD)
    own_v = values.reshape(kblocks, KB, HD)
    lse = logsum.reshape(qblocks, QB, heads).transpose(0, 2, 1).reshape(qblocks * heads // 2, 2 * QB)
    terms = (shape((peers, KB, HD), BF16), shape((kblocks, KB, HD), F32))
    work = [
        pltpu.VMEM((span, HD), jnp.int32),
        pltpu.VMEM((heads * QB, HD), BF16),
        pltpu.VMEM((peers + kblocks, KB, HD), F32),
        pltpu.VMEM((qblocks, span, HD), F32),
    ]

    def home(came, peer):
        return call(
            functools.partial(gather_home, nq, nz),
            shape((nz * kblocks, KB, HD), BF16),
            "ss" + "v" * len(came),
            [pltpu.VMEM((nz * kblocks + 1, KB, HD), F32)],
        )(asked, peer, *came).reshape(nz, tok, HD)

    sent_v, mine_v = call(
        functools.partial(value_terms, nq, nz),
        terms,
        "ssvvvvv",
        [pltpu.VMEM((span, HD), BF16), work[0], pltpu.VMEM((span, heads * QB), BF16), *work[1:]],
    )(names, me, queries, out_grad, lse, got_k, own_k)
    came_v = to_peers(sent_v.reshape(nq, nz * KB, HD), XC).reshape(peers, KB, HD)
    dense_v = home([came_v], direct)
    sums_v = to_peers(dense_v, "z")
    value_grad = mine_v.reshape(tok, HD) + jnp.sum(sums_v.astype(F32), axis=0)

    *sent_k, mine_k, low, sel = call(
        functools.partial(key_terms, nx, nc, nz),
        (
            *(slab,) * nq,
            terms[1],
            shape((qblocks, span, heads * QB), BF16),
            shape((qblocks, span, HD), BF16),
        ),
        "ss" + "v" * (6 + nq),
        [pltpu.VMEM((span, HD), BF16), *work, pltpu.VMEM((peers, KB, HD), BF16)],
    )(names, me, queries, out_grad, lse, got_k, own_k, own_v, *got_v)
    came_k = around(sent_k)
    dense_k = home(came_k, behind)
    query_grad = call(query_terms, shape((tok, cols), F32), "vv")(low, sel)

    all_low = lax.all_gather(value_grad.astype(BF16), XC, axis=0)
    both = call(
        functools.partial(weight_terms, rows_out),
        shape((nz, tok + rows_out, HD), BF16),
        "v" * (2 + tp) + "s",
    )(all_low, dense_k, *planes, order)
    both = jnp.sum(to_peers(both, "z").astype(F32), axis=0)
    key_grad = mine_k.reshape(tok, HD) + both[:tok]
    return (query_grad, key_grad, value_grad, both[tok:])


def solution(mesh):
    kv, tp = mesh.shape["kv"], mesh.shape["tp"]
    split = Mesh(mesh.devices.reshape(kv // 8, 4, 2, tp), ("z", "x", "c", "tp"))
    cut = P(KV, "tp")

    return jax.shard_map(
        local,
        mesh=split,
        in_specs=(cut, cut, cut, cut, cut, cut, P(KV, None)),
        out_specs=(cut, cut, cut, cut),
        check_vma=False,
    )
```

```python
import functools

import jax
import jax.numpy as jnp
from jax import lax
from jax.experimental import pallas as pl
from jax.experimental.pallas import tpu as pltpu
from jax.sharding import Mesh
from jax.sharding import PartitionSpec as P

HD = 128
QB = 64
KB = 32
NSEL = 16
KV = ("z", "x", "c")
XC = ("x", "c")
SUB = 8
SCALE = HD ** (-0.5)
F32 = jnp.float32
BF16 = jnp.bfloat16
NT = (((1,), (1,)), ((), ()))
TN = (((0,), (0,)), ((), ()))


def to_peers(parts, axis):
    return lax.all_to_all(parts, axis, split_axis=0, concat_axis=0, tiled=True)


def smem():
    return pl.BlockSpec(memory_space=pltpu.SMEM)


def vmem():
    return pl.BlockSpec(memory_space=pltpu.VMEM)


def hbm():
    return pl.BlockSpec(memory_space=pltpu.HBM)


SPECS = {"s": smem, "v": vmem, "h": hbm}


def dma(n):
    return pltpu.SemaphoreType.DMA((n,))


def moves(pairs, sems):
    copies = [pltpu.make_async_copy(a, b, sems.at[i]) for i, (a, b) in enumerate(pairs)]
    for copy in copies:
        copy.start()
    return copies


def call(body, outs, ins, scratch=(), mib=60, to="v"):
    many = isinstance(outs, tuple)
    kinds = [SPECS[t]() for t in (to if many else to[0])]
    return pl.pallas_call(
        body,
        out_shape=outs,
        in_specs=[SPECS[i]() for i in ins],
        out_specs=tuple(kinds) if many else kinds[0],
        scratch_shapes=list(scratch),
        compiler_params=pltpu.CompilerParams(vmem_limit_bytes=mib * 1024 * 1024),
    )


def pick(nq, nz, asked, column, target, out, sems):
    kblocks = column.shape[0] // nz
    for q in range(nq):
        for z in range(nz):
            block = jnp.maximum(asked[q * 2 * nz + z] - 1, 0)
            out[q * nz + z] = column[z * kblocks + block]
        part = slice(q * nz, (q + 1) * nz)
        pltpu.make_async_copy(out.at[part], target.at[part], sems.at[q]).start()
    for q in range(nq):
        part = slice(q * nz, (q + 1) * nz)
        pltpu.make_async_copy(out.at[part], target.at[part], sems.at[q]).wait()


def pick_apart(nz, asked, ahead, column, other, *refs):
    *targets, outs, sems = refs
    kblocks = column.shape[0] // nz
    for s, target in enumerate(targets):
        out = outs.at[s]
        first = ahead[s] * 2 * nz
        for i in range(2 * nz):
            source = other if i >= nz else column
            block = jnp.maximum(asked[first + i] - 1, 0)
            out[i] = source[i % nz * kblocks + block]
        pltpu.make_async_copy(out, target, sems.at[s]).start()
    for s, target in enumerate(targets):
        pltpu.make_async_copy(outs.at[s], target, sems.at[s]).wait()


def by_feature(nq, nz, rows, chosen, here, features, out):
    tok, cols = features.shape
    kblocks = tok // KB
    for i in range(cols // HD):
        tile = features[:, i * HD : (i + 1) * HD].T
        for j in range(HD // rows):
            piece = i * (HD // rows) + j
            out[piece % nq, (piece // nq) * rows : (piece // nq + 1) * rows] = tile[
                j * rows : (j + 1) * rows
            ]
    at = lax.broadcasted_iota(jnp.int32, (nq, HD), 0) * HD + lax.broadcasted_iota(
        jnp.int32, (nq, HD), 1
    )
    wanted = jnp.zeros((nq, HD), F32)
    for e in range(chosen.shape[0]):
        c = chosen[e]
        owner = c // kblocks
        place = jnp.where(owner != here[0], (owner % nq) * HD + owner // nq, -1)
        pair = jnp.where(owner != here[0], (owner % nq ^ 1) * HD + nz + owner // nq, -1)
        block = (c % kblocks + 1).astype(F32)
        wanted = jnp.where((at == place) | (at == pair), block, wanted)
    wanted = wanted.astype(BF16)
    for q in range(nq):
        out[q, cols // nq :] = jnp.broadcast_to(wanted[q : q + 1], (SUB, HD))


def slots_of(chosen, here, b, nq, nz, kblocks, where):
    slots = []
    for e in range(NSEL):
        c = chosen[b * NSEL + e]
        owner = c // kblocks
        place = where(owner % nq) * nz + owner // nq
        slots.append((c, owner != here, place, c % kblocks))
    return slots


def select(slots, got, own, out):
    for e, (_, remote, place, within) in enumerate(slots):
        near = own[within]
        if isinstance(got, tuple):
            size = got[0].shape[0]
            step, at = place // size, place % size
            block = got[0][at]
            for i in range(1, len(got)):
                block = jnp.where(step == i, got[i][at], block)
        else:
            block = got[jnp.where(remote, place, 0)]
        out[e * KB : (e + 1) * KB] = jnp.where(remote, block, near)


def heads_of(ref, b, p):
    rows = slice(b * QB, (b + 1) * QB)
    return jnp.concatenate(
        [ref[rows, (2 * p + i) * HD : (2 * p + i + 1) * HD] for i in range(2)], axis=0
    )


def set_positions(slots, kpos):
    rows = lax.broadcasted_iota(jnp.int32, (KB, HD), 0)
    lanes = lax.broadcasted_iota(jnp.int32, (KB, HD), 1) % QB
    for e, (c, _, _, _) in enumerate(slots):
        kpos[e * KB : (e + 1) * KB] = c * KB + rows - lanes


def prob_of(sel, pair, lse, kpos, start, b, p, pairs):
    scores = lax.dot_general(sel[...], pair, NT, preferred_element_type=F32) * SCALE
    at = b * pairs + p
    return jnp.where(kpos[...] <= start, jnp.exp(scores - lse[at : at + 1, :]), 0.0)


def scatter(slots, parts, total, send, own_sum, peers, kblocks):
    def put(slot):
        _, remote, place, within = slot
        return jnp.where(remote, place, peers + within)

    zero = jnp.zeros((KB, HD), F32)
    for k in range(kblocks):
        total[peers + k] = zero
    for slot in slots[1]:
        total[put(slot)] = zero
    for b, part in enumerate(parts):
        for e, slot in enumerate(slots[b]):
            piece = part[e * KB : (e + 1) * KB]
            at = put(slot)
            total[at] = total[at] + piece if b else piece
    for b in range(len(parts)):
        for _, remote, place, _ in slots[b]:

            @pl.when(remote)
            def _(place=place):
                send[place] = total[place].astype(BF16)

    for k in range(kblocks):
        own_sum[k] = total[peers + k]


def value_terms(nq, nz, chosen, here, queries, dout, lse, got_k, own_k, target, own_sum, sel, kpos, low, rows, total, part, send, sems):
    peers, kblocks = nq * nz, own_k.shape[0]
    qblocks, pairs = queries.shape[0] // QB, queries.shape[1] // HD // 2
    slots = [slots_of(chosen, here[0], b, nq, nz, kblocks, lambda q: q) for b in range(qblocks)]
    for b in range(qblocks):
        select(slots[b], got_k, own_k, sel)
        set_positions(slots[b], kpos)
        start = here[0] * queries.shape[0] + b * QB
        for p in range(pairs):
            pair = heads_of(queries, b, p)
            prob = prob_of(sel, pair, lse, kpos, start, b, p, pairs)
            low[:, p * HD : (p + 1) * HD] = prob.astype(BF16)
            rows[p * HD : (p + 1) * HD] = heads_of(dout, b, p)
        part[b] = jnp.dot(low[...], rows[...], preferred_element_type=F32)
    scatter(slots, [part.at[b] for b in range(qblocks)], total, send, own_sum, peers, kblocks)
    for copy in moves([(send, target)], sems):
        copy.wait()


def key_terms(nx, nc, nz, chosen, here, queries, dout, lse, got_k, own_k, own_v, *refs):
    nq = nx * nc
    far_v, refs = refs[:nx], refs[nx:]
    targets, refs = refs[:nx], refs[nx:]
    own_sum, low, sel, sel_v, kpos, rows, total, part, send, held, sems = refs
    got_v = tuple(held.at[s] for s in range(nx))
    for copy in moves(list(zip(far_v, got_v)), sems):
        copy.wait()
    peers, kblocks = nq * nz, own_k.shape[0]
    qblocks, pairs = queries.shape[0] // QB, queries.shape[1] // HD // 2
    mine = here[0] % nq

    def behind(q):
        return (mine // nc - q // nc) % nx * nc + (mine + q) % nc

    def ahead(q):
        return (q // nc - mine // nc) % nx * nc + (mine + q) % nc

    def slots(b, where):
        return slots_of(chosen, here[0], b, nq, nz, kblocks, where)

    for b in range(qblocks):
        select(slots(b, lambda q: q), got_k, own_k, sel.at[b])
        select(slots(b, behind), got_v, own_v, sel_v)
        set_positions(slots(b, ahead), kpos)
        start = here[0] * queries.shape[0] + b * QB
        for p in range(pairs):
            pair = heads_of(queries, b, p)
            prob = prob_of(sel.at[b], pair, lse, kpos, start, b, p, pairs)
            dprob = lax.dot_general(sel_v[...], heads_of(dout, b, p), NT, preferred_element_type=F32)
            delta = jnp.sum(prob * dprob, axis=0, keepdims=True)
            low[b, :, p * HD : (p + 1) * HD] = (prob * (dprob - delta)).astype(BF16)
            rows[p * HD : (p + 1) * HD] = pair
        part[b] = jnp.dot(low[b], rows[...], preferred_element_type=F32) * SCALE
    back = [slots(b, ahead) for b in range(qblocks)]
    scatter(back, [part.at[b] for b in range(qblocks)], total, send, own_sum, peers, kblocks)
    size = nc * nz
    ends = [(send.at[s * size : (s + 1) * size], to) for s, to in enumerate(targets)]
    for copy in moves(ends, sems):
        copy.wait()


def query_terms(low, sel, out):
    for b in range(low.shape[0]):
        for p in range(low.shape[2] // HD):
            got = lax.dot_general(
                low[b, :, p * HD : (p + 1) * HD], sel[b], TN, preferred_element_type=F32
            )
            for i in range(2):
                out[b * QB : (b + 1) * QB, (2 * p + i) * HD : (2 * p + i + 1) * HD] = (
                    got[i * QB : (i + 1) * QB] * SCALE
                )


def gather_home(nq, nz, asked, came, dense, total):
    blocks = dense.shape[0]
    kblocks = blocks // nz
    total[...] = jnp.zeros_like(total)
    for q in range(nq):
        for z in range(nz):
            a = asked[q * 2 * nz + z]
            at = jnp.where(a > 0, z * kblocks + a - 1, blocks)
            total[at] = total[at] + came[q * nz + z].astype(F32)
    dense[...] = total[0:blocks].astype(BF16)


def gather_both(nz, asked, behind, *refs):
    *sent, dense, target, total, came, other, sems = refs
    copies = moves([(a, came.at[s]) for s, a in enumerate(sent)], sems)
    blocks = dense.shape[0]
    kblocks = blocks // nz
    total[...] = jnp.zeros_like(total)
    for s, copy in enumerate(copies):
        copy.wait()
        part = came.at[s]
        first = behind[s] * 2 * nz
        for i in range(2 * nz):
            a = asked[first + i]
            at = jnp.where(a > 0, i * kblocks + a - 1, 2 * blocks)
            total[at] = total[at] + part[i].astype(F32)
    other[...] = total[blocks : 2 * blocks].astype(BF16)
    copies = moves([(other, target)], sems)
    dense[...] = total[0:blocks]
    for copy in copies:
        copy.wait()


def weight_terms(rows_out, low, dense, other, *refs):
    *features, order, out = refs
    nq, nz, tok = low.shape[0], dense.shape[0], dense.shape[1]
    mine = nz // len(features)
    feats = mine * rows_out
    for k, block in enumerate(features):
        total = jnp.dot(block[0, 0:feats], low[0], preferred_element_type=F32)
        for q in range(1, nq):
            total = total + jnp.dot(block[q, 0:feats], low[q], preferred_element_type=F32)
        total = total.astype(BF16)
        for a in range(mine):
            out[order[k] * mine + a, tok:] = total[a * rows_out : (a + 1) * rows_out]
    out[:, 0:tok] = (dense[...] + other[...].astype(F32)).astype(BF16)


def local(queries, keys, values, logsum, out_grad, normed_input, chosen):
    nz = lax.axis_size("z")
    nq = lax.axis_size(XC)
    tp = lax.axis_size("tp")
    here = lax.axis_index(KV)
    tok, cols = queries.shape
    kblocks = tok // KB
    qblocks = tok // QB
    heads = cols // HD
    span = NSEL * KB
    peers = nq * nz
    shape = jax.ShapeDtypeStruct

    names = chosen.reshape(qblocks * NSEL)
    me = here.reshape(1).astype(jnp.int32)

    rows_out = normed_input.shape[1] * tp // peers
    mine = nz // tp
    feats = mine * rows_out
    split = call(
        functools.partial(by_feature, nq, nz, rows_out),
        shape((nq, feats + SUB, tok), BF16),
        "ssv",
    )(names, me, normed_input)
    split = to_peers(split, XC)
    asked = split[:, feats, : 2 * nz].astype(jnp.int32).reshape(2 * peers)
    planes = [split]
    for k in range(1, tp):
        planes.append(lax.ppermute(planes[0], "tp", [(i, (i + k) % tp) for i in range(tp)]))
    order = ((lax.axis_index("tp") - jnp.arange(tp)) % tp).astype(jnp.int32)
    nx, nc = lax.axis_size("x"), lax.axis_size("c")
    steps = jnp.arange(nx)
    my_x, my_c = lax.axis_index("x"), lax.axis_index("c")
    ahead = ((my_x + steps) % nx * nc + my_c).astype(jnp.int32)
    behind = ((my_x - steps) % nx * nc + my_c).astype(jnp.int32)

    def around(pieces):
        turns = [[(x, (x + s) % nx) for x in range(nx)] for s in range(nx)]
        return [pieces[0]] + [lax.ppermute(pieces[s], "x", turns[s]) for s in range(1, nx)]

    def swapped(rows):
        return lax.ppermute(rows, "c", [(0, 1), (1, 0)])

    def column(rows):
        return lax.all_gather(rows, "z", axis=0, tiled=True).reshape(nz * kblocks, KB, HD)

    column_k = column(keys)
    sent = call(
        functools.partial(pick, nq, nz),
        shape((peers, KB, HD), BF16),
        "sv",
        [pltpu.VMEM((peers, KB, HD), BF16), dma(nq)],
        to="h",
    )(asked, column_k)
    got_k = to_peers(sent.reshape(nq, nz * KB, HD), XC).reshape(peers, KB, HD)
    column_v = column(values)
    other_v = swapped(column_v)
    slab = shape((nc * nz, KB, HD), BF16)
    sent = call(
        functools.partial(pick_apart, nz),
        (slab,) * nx,
        "ssvv",
        [pltpu.VMEM((nx, nc * nz, KB, HD), BF16), dma(nx)],
        to="h" * nx,
    )(asked, ahead, column_v, other_v)
    got_v = around(sent)

    own_k = keys.reshape(kblocks, KB, HD)
    own_v = values.reshape(kblocks, KB, HD)
    lse = logsum.reshape(qblocks, QB, heads).transpose(0, 2, 1).reshape(qblocks * heads // 2, 2 * QB)
    terms = (shape((peers, KB, HD), BF16), shape((kblocks, KB, HD), F32))
    slots = pltpu.VMEM((peers, KB, HD), BF16)
    work = [
        pltpu.VMEM((span, HD), jnp.int32),
        pltpu.VMEM((heads * QB, HD), BF16),
        pltpu.VMEM((peers + kblocks, KB, HD), F32),
        pltpu.VMEM((qblocks, span, HD), F32),
    ]

    sent_v, mine_v = call(
        functools.partial(value_terms, nq, nz),
        terms,
        "ssvvvvv",
        [pltpu.VMEM((span, HD), BF16), work[0], pltpu.VMEM((span, heads * QB), BF16), *work[1:], slots, dma(1)],
        to="hv",
    )(names, me, queries, out_grad, lse, got_k, own_k)
    came_v = to_peers(sent_v.reshape(nq, nz * KB, HD), XC).reshape(peers, KB, HD)
    dense_v = call(
        functools.partial(gather_home, nq, nz),
        shape((nz * kblocks, KB, HD), BF16),
        "sv",
        [pltpu.VMEM((nz * kblocks + 1, KB, HD), F32)],
        6,
    )(asked, came_v).reshape(nz, tok, HD)
    sums_v = to_peers(dense_v, "z")
    value_grad = mine_v.reshape(tok, HD) + jnp.sum(sums_v.astype(F32), axis=0)

    *sent_k, mine_k, low, sel = call(
        functools.partial(key_terms, nx, nc, nz),
        (
            *(slab,) * nx,
            terms[1],
            shape((qblocks, span, heads * QB), BF16),
            shape((qblocks, span, HD), BF16),
        ),
        "ss" + "v" * 6 + "h" * nx,
        [
            *(pltpu.VMEM((span, HD), BF16), *work, slots),
            *(pltpu.VMEM((nx, nc * nz, KB, HD), BF16), dma(nx)),
        ],
        to="h" * nx + "vvv",
    )(names, me, queries, out_grad, lse, got_k, own_k, own_v, *got_v)
    came_k = around(sent_k)
    blocks = (nz * kblocks, KB, HD)
    dense_k, other_k = call(
        functools.partial(gather_both, nz),
        (shape(blocks, F32), shape(blocks, BF16)),
        "ss" + "h" * nx,
        [
            pltpu.VMEM((2 * nz * kblocks + 1, KB, HD), F32),
            pltpu.VMEM((nx, nc * nz, KB, HD), BF16),
            pltpu.VMEM(blocks, BF16),
            dma(nx),
        ],
        to="vh",
    )(asked, behind, *came_k)
    other_k = swapped(other_k)
    query_grad = call(query_terms, shape((tok, cols), F32), "vv")(low, sel)

    all_low = lax.all_gather(value_grad.astype(BF16), XC, axis=0)
    both = call(
        functools.partial(weight_terms, rows_out),
        shape((nz, tok + rows_out, HD), BF16),
        "v" * (3 + tp) + "s",
        mib=6,
    )(
        all_low, dense_k.reshape(nz, tok, HD), other_k.reshape(nz, tok, HD), *planes, order
    )
    both = jnp.sum(to_peers(both, "z").astype(F32), axis=0)
    key_grad = mine_k.reshape(tok, HD) + both[:tok]
    return (query_grad, key_grad, value_grad, both[tok:])


def solution(mesh):
    kv, tp = mesh.shape["kv"], mesh.shape["tp"]
    split = Mesh(mesh.devices.reshape(kv // 8, 4, 2, tp), ("z", "x", "c", "tp"))
    cut = P(KV, "tp")

    return jax.shard_map(
        local,
        mesh=split,
        in_specs=(cut, cut, cut, cut, cut, cut, P(KV, None)),
        out_specs=(cut, cut, cut, cut),
        check_vma=False,
    )
```

```python
import functools

import jax
import jax.numpy as jnp
from jax import lax
from jax.experimental import pallas as pl
from jax.experimental.pallas import tpu as pltpu
from jax.sharding import Mesh
from jax.sharding import PartitionSpec as P

HD = 128
QB = 64
KB = 32
NSEL = 16
KV = ("z", "x", "c")
XC = ("x", "c")
SUB = 8
SCALE = HD ** (-0.5)
F32 = jnp.float32
BF16 = jnp.bfloat16
NT = (((1,), (1,)), ((), ()))
TN = (((0,), (0,)), ((), ()))


def to_peers(parts, axis):
    return lax.all_to_all(parts, axis, split_axis=0, concat_axis=0, tiled=True)


def smem():
    return pl.BlockSpec(memory_space=pltpu.SMEM)


def vmem():
    return pl.BlockSpec(memory_space=pltpu.VMEM)


def hbm():
    return pl.BlockSpec(memory_space=pltpu.HBM)


SPECS = {"s": smem, "v": vmem, "h": hbm}


def dma(n):
    return pltpu.SemaphoreType.DMA((n,))


def moves(pairs, sems):
    copies = [pltpu.make_async_copy(a, b, sems.at[i]) for i, (a, b) in enumerate(pairs)]
    for copy in copies:
        copy.start()
    return copies


def call(body, outs, ins, scratch=(), mib=60, to="v"):
    many = isinstance(outs, tuple)
    kinds = [SPECS[t]() for t in (to if many else to[0])]
    return pl.pallas_call(
        body,
        out_shape=outs,
        in_specs=[SPECS[i]() for i in ins],
        out_specs=tuple(kinds) if many else kinds[0],
        scratch_shapes=list(scratch),
        compiler_params=pltpu.CompilerParams(vmem_limit_bytes=mib * 1024 * 1024),
    )


def pick(nq, nz, asked, column, target, out, sems):
    kblocks = column.shape[0] // nz
    for q in range(nq):
        for z in range(nz):
            block = jnp.maximum(asked[q, z] - 1, 0)
            out[q * nz + z] = column[z * kblocks + block]
        part = slice(q * nz, (q + 1) * nz)
        pltpu.make_async_copy(out.at[part], target.at[part], sems.at[q]).start()
    for q in range(nq):
        part = slice(q * nz, (q + 1) * nz)
        pltpu.make_async_copy(out.at[part], target.at[part], sems.at[q]).wait()


def across(here, s, nx, nc):
    mine = here % (nx * nc)
    return (mine // nc + s + nx) % nx * nc + mine % nc


def pick_apart(nc, nz, asked, here, column, other, *refs):
    *targets, outs, sems = refs
    nx = len(targets)
    kblocks = column.shape[0] // nz
    for s, target in enumerate(targets):
        out = outs.at[s]
        peer = across(here[0], s, nx, nc)
        for i in range(2 * nz):
            source = other if i >= nz else column
            block = jnp.maximum(asked[peer, i] - 1, 0)
            out[i] = source[i % nz * kblocks + block]
        pltpu.make_async_copy(out, target, sems.at[s]).start()
    for s, target in enumerate(targets):
        pltpu.make_async_copy(outs.at[s], target, sems.at[s]).wait()


def by_feature(nq, nz, rows, chosen, here, features, out):
    tok, cols = features.shape
    kblocks = tok // KB
    for i in range(cols // HD):
        tile = features[:, i * HD : (i + 1) * HD].T
        for j in range(HD // rows):
            piece = i * (HD // rows) + j
            out[piece % nq, (piece // nq) * rows : (piece // nq + 1) * rows] = tile[
                j * rows : (j + 1) * rows
            ]
    at = lax.broadcasted_iota(jnp.int32, (nq, HD), 0) * HD + lax.broadcasted_iota(
        jnp.int32, (nq, HD), 1
    )
    wanted = jnp.zeros((nq, HD), F32)
    for e in range(chosen.shape[0] * NSEL):
        c = chosen[e // NSEL, e % NSEL]
        owner = c // kblocks
        place = jnp.where(owner != here[0], (owner % nq) * HD + owner // nq, -1)
        pair = jnp.where(owner != here[0], (owner % nq ^ 1) * HD + nz + owner // nq, -1)
        block = (c % kblocks + 1).astype(F32)
        wanted = jnp.where((at == place) | (at == pair), block, wanted)
    wanted = wanted.astype(BF16)
    for q in range(nq):
        out[q, cols // nq :] = jnp.broadcast_to(wanted[q : q + 1], (SUB, HD))


def slots_of(chosen, here, b, nq, nz, kblocks, where):
    slots = []
    for e in range(NSEL):
        c = chosen[b, e]
        owner = c // kblocks
        place = where(owner % nq) * nz + owner // nq
        slots.append((c, owner != here, place, c % kblocks))
    return slots


def select(slots, got, own, out):
    for e, (_, remote, place, within) in enumerate(slots):
        near = own[within]
        if isinstance(got, tuple):
            size = got[0].shape[0]
            step, at = place // size, place % size
            block = got[0][at]
            for i in range(1, len(got)):
                block = jnp.where(step == i, got[i][at], block)
        else:
            block = got[jnp.where(remote, place, 0)]
        out[e * KB : (e + 1) * KB] = jnp.where(remote, block, near)


def heads_of(ref, b, p):
    rows = slice(b * QB, (b + 1) * QB)
    return jnp.concatenate(
        [ref[rows, (2 * p + i) * HD : (2 * p + i + 1) * HD] for i in range(2)], axis=0
    )


def set_positions(slots, kpos):
    rows = lax.broadcasted_iota(jnp.int32, (KB, HD), 0)
    lanes = lax.broadcasted_iota(jnp.int32, (KB, HD), 1) % QB
    for e, (c, _, _, _) in enumerate(slots):
        kpos[e * KB : (e + 1) * KB] = c * KB + rows - lanes


def prob_of(sel, pair, lse, kpos, start, b, p):
    scores = lax.dot_general(sel[...], pair, NT, preferred_element_type=F32) * SCALE
    turned = pltpu.roll(lse[...], QB, 1)
    left, right = (turned, lse[...]) if b else (lse[...], turned)
    first = lax.broadcasted_iota(jnp.int32, (1, HD), 1) < QB
    row = jnp.where(first, left[2 * p : 2 * p + 1], right[2 * p + 1 : 2 * p + 2])
    return jnp.where(kpos[...] <= start, jnp.exp(scores - row), 0.0)


def scatter(slots, parts, total, send, own_sum, peers, kblocks):
    def put(slot):
        _, remote, place, within = slot
        return jnp.where(remote, place, peers + within)

    zero = jnp.zeros((KB, HD), F32)
    for k in range(kblocks):
        total[peers + k] = zero
    for slot in slots[1]:
        total[put(slot)] = zero
    for b, part in enumerate(parts):
        for e, slot in enumerate(slots[b]):
            piece = part[e * KB : (e + 1) * KB]
            at = put(slot)
            total[at] = total[at] + piece if b else piece
    for b in range(len(parts)):
        for _, remote, place, _ in slots[b]:

            @pl.when(remote)
            def _(place=place):
                send[place] = total[place].astype(BF16)

    for k in range(kblocks):
        own_sum[k] = total[peers + k]


def value_terms(nq, nz, chosen, here, queries, dout, lse, got_k, own_k, target, own_sum, sel, kpos, low, rows, total, part, send, sems):
    peers, kblocks = nq * nz, own_k.shape[0]
    qblocks, pairs = queries.shape[0] // QB, queries.shape[1] // HD // 2
    slots = [slots_of(chosen, here[0], b, nq, nz, kblocks, lambda q: q) for b in range(qblocks)]
    for b in range(qblocks):
        select(slots[b], got_k, own_k, sel)
        set_positions(slots[b], kpos)
        start = here[0] * queries.shape[0] + b * QB
        for p in range(pairs):
            pair = heads_of(queries, b, p)
            prob = prob_of(sel, pair, lse, kpos, start, b, p)
            low[:, p * HD : (p + 1) * HD] = prob.astype(BF16)
            rows[p * HD : (p + 1) * HD] = heads_of(dout, b, p)
        part[b] = jnp.dot(low[...], rows[...], preferred_element_type=F32)
    scatter(slots, [part.at[b] for b in range(qblocks)], total, send, own_sum, peers, kblocks)
    for copy in moves([(send, target)], sems):
        copy.wait()


def key_terms(nx, nc, nz, chosen, here, lse, own_k, own_v, *refs):
    nq = nx * nc
    ins, refs = refs[: 3 + nx], refs[3 + nx :]
    targets, refs = refs[:nx], refs[nx:]
    own_sum, low, sel, sel_v, kpos, rows, total, part, send, held, queries, dout, got_k, sems = refs
    got_v = tuple(held.at[s] for s in range(nx))
    for copy in moves(list(zip(ins, (queries, dout, got_k, *got_v))), sems):
        copy.wait()
    peers, kblocks = nq * nz, own_k.shape[0]
    qblocks, pairs = queries.shape[0] // QB, queries.shape[1] // HD // 2
    mine = here[0] % nq

    def behind(q):
        return (mine // nc - q // nc) % nx * nc + (mine + q) % nc

    def ahead(q):
        return (q // nc - mine // nc) % nx * nc + (mine + q) % nc

    def slots(b, where):
        return slots_of(chosen, here[0], b, nq, nz, kblocks, where)

    for b in range(qblocks):
        select(slots(b, lambda q: q), got_k, own_k, sel.at[b])
        select(slots(b, behind), got_v, own_v, sel_v)
        set_positions(slots(b, ahead), kpos)
        start = here[0] * queries.shape[0] + b * QB
        for p in range(pairs):
            pair = heads_of(queries, b, p)
            prob = prob_of(sel.at[b], pair, lse, kpos, start, b, p)
            dprob = lax.dot_general(sel_v[...], heads_of(dout, b, p), NT, preferred_element_type=F32)
            delta = jnp.sum(prob * dprob, axis=0, keepdims=True)
            low[b, :, p * HD : (p + 1) * HD] = (prob * (dprob - delta)).astype(BF16)
            rows[p * HD : (p + 1) * HD] = pair
        part[b] = jnp.dot(low[b], rows[...], preferred_element_type=F32) * SCALE
    back = [slots(b, ahead) for b in range(qblocks)]
    scatter(back, [part.at[b] for b in range(qblocks)], total, send, own_sum, peers, kblocks)
    size = nc * nz
    ends = [(send.at[s * size : (s + 1) * size], to) for s, to in enumerate(targets)]
    for copy in moves(ends, sems):
        copy.wait()


def query_terms(low, sel, out):
    for b in range(low.shape[0]):
        for p in range(low.shape[2] // HD):
            got = lax.dot_general(
                low[b, :, p * HD : (p + 1) * HD], sel[b], TN, preferred_element_type=F32
            )
            for i in range(2):
                out[b * QB : (b + 1) * QB, (2 * p + i) * HD : (2 * p + i + 1) * HD] = (
                    got[i * QB : (i + 1) * QB] * SCALE
                )


def gather_home(nq, nz, asked, came, dense, total):
    blocks = dense.shape[0]
    kblocks = blocks // nz
    total[...] = jnp.zeros_like(total)
    for q in range(nq):
        for z in range(nz):
            a = asked[q, z]
            at = jnp.where(a > 0, z * kblocks + a - 1, blocks)
            total[at] = total[at] + came[q * nz + z].astype(F32)
    dense[...] = total[0:blocks].astype(BF16)


def gather_both(nc, nz, asked, here, *refs):
    *sent, dense, target, total, came, other, sems = refs
    copies = moves([(a, came.at[s]) for s, a in enumerate(sent)], sems)
    blocks = dense.shape[0]
    kblocks = blocks // nz
    total[...] = jnp.zeros_like(total)
    for s, copy in enumerate(copies):
        copy.wait()
        part = came.at[s]
        peer = across(here[0], -s, len(sent), nc)
        for i in range(2 * nz):
            a = asked[peer, i]
            at = jnp.where(a > 0, i * kblocks + a - 1, 2 * blocks)
            total[at] = total[at] + part[i].astype(F32)
    other[...] = total[blocks : 2 * blocks].astype(BF16)
    copies = moves([(other, target)], sems)
    dense[...] = total[0:blocks]
    for copy in copies:
        copy.wait()


def weight_terms(rows_out, low, dense, other, *refs):
    *features, order, out = refs
    nq, nz, tok = low.shape[0], dense.shape[0], dense.shape[1]
    mine = nz // (2 * len(features))
    feats = mine * rows_out
    for k, block in enumerate(f.at[i] for f in features for i in range(2)):
        total = jnp.dot(block[0, 0:feats], low[0], preferred_element_type=F32)
        for q in range(1, nq):
            total = total + jnp.dot(block[q, 0:feats], low[q], preferred_element_type=F32)
        total = total.astype(BF16)
        for a in range(mine):
            out[order[k] * mine + a, tok:] = total[a * rows_out : (a + 1) * rows_out]
    out[:, 0:tok] = (dense[...] + other[...].astype(F32)).astype(BF16)


def local(queries, keys, values, logsum, out_grad, normed_input, chosen):
    nz = lax.axis_size("z")
    nq = lax.axis_size(XC)
    tp = lax.axis_size("tp")
    here = lax.axis_index(KV)
    tok, cols = queries.shape
    kblocks = tok // KB
    qblocks = tok // QB
    heads = cols // HD
    span = NSEL * KB
    peers = nq * nz
    shape = jax.ShapeDtypeStruct

    names = chosen
    me = here.reshape(1).astype(jnp.int32)

    rows_out = normed_input.shape[1] * tp // peers
    mine = nz // tp
    feats = mine * rows_out
    split = call(
        functools.partial(by_feature, nq, nz, rows_out),
        shape((nq, feats + SUB, tok), BF16),
        "ssv",
    )(names, me, normed_input)
    split = to_peers(split, XC)
    asked = split[:, feats, : 2 * nz].astype(jnp.int32)
    pairs = [(i, i ^ 1) for i in range(tp)]
    cross = [(i, (i + 1 if i % 2 else i - 1) % tp) for i in range(tp)]
    my_t = lax.axis_index("tp")
    near = lax.ppermute(split, "tp", pairs)
    held = jnp.stack([split, near])
    names_of = jnp.stack([my_t, my_t ^ 1])
    planes, order = [held], [names_of]
    if tp > 2:
        planes.append(lax.ppermute(held, "tp", cross))
        over = jnp.where(my_t % 2 == 1, my_t + 1, my_t - 1 + tp) % tp
        order.append(jnp.stack([over, over ^ 1]))
    order = jnp.concatenate(order).astype(jnp.int32)
    nx, nc = lax.axis_size("x"), lax.axis_size("c")

    def around(pieces):
        turns = [[(x, (x + s) % nx) for x in range(nx)] for s in range(nx)]
        return [pieces[0]] + [lax.ppermute(pieces[s], "x", turns[s]) for s in range(1, nx)]

    def swapped(rows):
        return lax.ppermute(rows, "c", [(0, 1), (1, 0)])

    def column(rows):
        return lax.all_gather(rows, "z", axis=0, tiled=True).reshape(nz * kblocks, KB, HD)

    column_k = column(keys)
    sent = call(
        functools.partial(pick, nq, nz),
        shape((peers, KB, HD), BF16),
        "sv",
        [pltpu.VMEM((peers, KB, HD), BF16), dma(nq)],
        to="h",
    )(asked, column_k)
    got_k = to_peers(sent.reshape(nq, nz * KB, HD), XC).reshape(peers, KB, HD)
    column_v = column(values)
    other_v = swapped(column_v)
    slab = shape((nc * nz, KB, HD), BF16)
    sent = call(
        functools.partial(pick_apart, nc, nz),
        (slab,) * nx,
        "ssvv",
        [pltpu.VMEM((nx, nc * nz, KB, HD), BF16), dma(nx)],
        to="h" * nx,
    )(asked, me, column_v, other_v)
    got_v = around(sent)

    own_k = keys.reshape(kblocks, KB, HD)
    own_v = values.reshape(kblocks, KB, HD)
    lse = logsum.T
    terms = (shape((peers, KB, HD), BF16), shape((kblocks, KB, HD), F32))
    slots = pltpu.VMEM((peers, KB, HD), BF16)
    rows = pltpu.VMEM((tok, cols), BF16)
    work = [
        pltpu.VMEM((span, HD), jnp.int32),
        pltpu.VMEM((heads * QB, HD), BF16),
        pltpu.VMEM((peers + kblocks, KB, HD), F32),
        pltpu.VMEM((qblocks, span, HD), F32),
    ]

    sent_v, mine_v = call(
        functools.partial(value_terms, nq, nz),
        terms,
        "ssvvvvv",
        [pltpu.VMEM((span, HD), BF16), work[0], pltpu.VMEM((span, heads * QB), BF16), *work[1:], slots, dma(1)],
        mib=8,
        to="hv",
    )(names, me, queries, out_grad, lse, got_k, own_k)
    came_v = to_peers(sent_v.reshape(nq, nz * KB, HD), XC).reshape(peers, KB, HD)
    dense_v = call(
        functools.partial(gather_home, nq, nz),
        shape((nz * kblocks, KB, HD), BF16),
        "sv",
        [pltpu.VMEM((nz * kblocks + 1, KB, HD), F32)],
        6,
    )(asked, came_v).reshape(nz, tok, HD)
    sums_v = to_peers(dense_v, "z")
    value_grad = mine_v.reshape(tok, HD) + jnp.sum(sums_v.astype(F32), axis=0)

    *sent_k, mine_k, low, sel = call(
        functools.partial(key_terms, nx, nc, nz),
        (
            *(slab,) * nx,
            terms[1],
            shape((qblocks, span, heads * QB), BF16),
            shape((qblocks, span, HD), BF16),
        ),
        "ssvvv" + "h" * (3 + nx),
        [
            *(pltpu.VMEM((span, HD), BF16), *work, slots),
            *(pltpu.VMEM((nx, nc * nz, KB, HD), BF16), rows, rows, slots, dma(3 + nx)),
        ],
        to="h" * nx + "vvv",
    )(names, me, lse, own_k, own_v, queries, out_grad, got_k, *got_v)
    came_k = around(sent_k)
    blocks = (nz * kblocks, KB, HD)
    dense_k, other_k = call(
        functools.partial(gather_both, nc, nz),
        (shape(blocks, F32), shape(blocks, BF16)),
        "ss" + "h" * nx,
        [
            pltpu.VMEM((2 * nz * kblocks + 1, KB, HD), F32),
            pltpu.VMEM((nx, nc * nz, KB, HD), BF16),
            pltpu.VMEM(blocks, BF16),
            dma(nx),
        ],
        to="vh",
    )(asked, me, *came_k)
    other_k = swapped(other_k)
    query_grad = call(query_terms, shape((tok, cols), F32), "vv")(low, sel)

    all_low = lax.all_gather(value_grad.astype(BF16), XC, axis=0)
    both = call(
        functools.partial(weight_terms, rows_out),
        shape((nz, tok + rows_out, HD), BF16),
        "v" * (3 + len(planes)) + "s",
        mib=6,
    )(
        all_low, dense_k.reshape(nz, tok, HD), other_k.reshape(nz, tok, HD), *planes, order
    )
    both = jnp.sum(to_peers(both, "z").astype(F32), axis=0)
    key_grad = mine_k.reshape(tok, HD) + both[:tok]
    return (query_grad, key_grad, value_grad, both[tok:])


def solution(mesh):
    kv, tp = mesh.shape["kv"], mesh.shape["tp"]
    split = Mesh(mesh.devices.reshape(kv // 8, 4, 2, tp), ("z", "x", "c", "tp"))
    cut = P(KV, "tp")

    return jax.shard_map(
        local,
        mesh=split,
        in_specs=(cut, cut, cut, cut, cut, cut, P(KV, None)),
        out_specs=(cut, cut, cut, cut),
        check_vma=False,
    )
```

```python
import functools

import jax
import jax.numpy as jnp
from jax import lax
from jax.experimental import pallas as pl
from jax.experimental.pallas import tpu as pltpu
from jax.sharding import Mesh
from jax.sharding import PartitionSpec as P

HD = 128
QB = 64
KB = 32
NSEL = 16
KV = ("z", "x", "c")
XC = ("x", "c")
SUB = 8
SCALE = HD ** (-0.5)
F32 = jnp.float32
BF16 = jnp.bfloat16
NT = (((1,), (1,)), ((), ()))
TN = (((0,), (0,)), ((), ()))


def to_peers(parts, axis):
    return lax.all_to_all(parts, axis, split_axis=0, concat_axis=0, tiled=True)


def smem():
    return pl.BlockSpec(memory_space=pltpu.SMEM)


def vmem():
    return pl.BlockSpec(memory_space=pltpu.VMEM)


def hbm():
    return pl.BlockSpec(memory_space=pltpu.HBM)


SPECS = {"s": smem, "v": vmem, "h": hbm}


def dma(n):
    return pltpu.SemaphoreType.DMA((n,))


def moves(pairs, sems):
    copies = [pltpu.make_async_copy(a, b, sems.at[i]) for i, (a, b) in enumerate(pairs)]
    for copy in copies:
        copy.start()
    return copies


def call(body, outs, ins, scratch=(), mib=60, to="v"):
    many = isinstance(outs, tuple)
    kinds = [SPECS[t]() for t in (to if many else to[0])]
    return pl.pallas_call(
        body,
        out_shape=outs,
        in_specs=[SPECS[i]() for i in ins],
        out_specs=tuple(kinds) if many else kinds[0],
        scratch_shapes=list(scratch),
        compiler_params=pltpu.CompilerParams(vmem_limit_bytes=mib * 1024 * 1024),
    )


def pick(nq, nz, asked, column, target, out, sems):
    kblocks = column.shape[0] // nz
    for q in range(nq):
        for z in range(nz):
            block = jnp.maximum(asked[q, z] - 1, 0)
            out[q * nz + z] = column[z * kblocks + block]
        part = slice(q * nz, (q + 1) * nz)
        pltpu.make_async_copy(out.at[part], target.at[part], sems.at[q]).start()
    for q in range(nq):
        part = slice(q * nz, (q + 1) * nz)
        pltpu.make_async_copy(out.at[part], target.at[part], sems.at[q]).wait()


def across(here, s, nx, nc):
    mine = here % (nx * nc)
    return (mine // nc + s + nx) % nx * nc + mine % nc


def pick_apart(nc, nz, asked, here, column, other, *refs):
    *targets, outs, sems = refs
    nx = len(targets)
    kblocks = column.shape[0] // nz
    for s, target in enumerate(targets):
        out = outs.at[s]
        peer = across(here[0], s, nx, nc)
        for i in range(2 * nz):
            source = other if i >= nz else column
            block = jnp.maximum(asked[peer, i] - 1, 0)
            out[i] = source[i % nz * kblocks + block]
        pltpu.make_async_copy(out, target, sems.at[s]).start()
    for s, target in enumerate(targets):
        pltpu.make_async_copy(outs.at[s], target, sems.at[s]).wait()


def by_feature(nq, nz, rows, chosen, here, features, out):
    tok, cols = features.shape
    kblocks = tok // KB
    for i in range(cols // HD):
        tile = features[:, i * HD : (i + 1) * HD].T
        for j in range(HD // rows):
            piece = i * (HD // rows) + j
            out[piece % nq, (piece // nq) * rows : (piece // nq + 1) * rows] = tile[
                j * rows : (j + 1) * rows
            ]
    at = lax.broadcasted_iota(jnp.int32, (nq, HD), 0) * HD + lax.broadcasted_iota(
        jnp.int32, (nq, HD), 1
    )
    wanted = jnp.zeros((nq, HD), F32)
    for e in range(chosen.shape[0] * NSEL):
        c = chosen[e // NSEL, e % NSEL]
        owner = c // kblocks
        place = jnp.where(owner != here[0], (owner % nq) * HD + owner // nq, -1)
        pair = jnp.where(owner != here[0], (owner % nq ^ 1) * HD + nz + owner // nq, -1)
        block = (c % kblocks + 1).astype(F32)
        wanted = jnp.where((at == place) | (at == pair), block, wanted)
    wanted = wanted.astype(BF16)
    for q in range(nq):
        out[q, cols // nq :] = jnp.broadcast_to(wanted[q : q + 1], (SUB, HD))


def slots_of(chosen, here, b, nq, nz, kblocks, where):
    slots = []
    for e in range(NSEL):
        c = chosen[b, e]
        owner = c // kblocks
        place = where(owner % nq) * nz + owner // nq
        slots.append((c, owner != here, place, c % kblocks))
    return slots


def select(slots, got, own, out):
    for e, (_, remote, place, within) in enumerate(slots):
        near = own[within]
        if isinstance(got, tuple):
            size = got[0].shape[0]
            step, at = place // size, place % size
            block = got[0][at]
            for i in range(1, len(got)):
                block = jnp.where(step == i, got[i][at], block)
        else:
            block = got[jnp.where(remote, place, 0)]
        out[e * KB : (e + 1) * KB] = jnp.where(remote, block, near)


def heads_of(ref, b, p):
    rows = slice(b * QB, (b + 1) * QB)
    return jnp.concatenate(
        [ref[rows, (2 * p + i) * HD : (2 * p + i + 1) * HD] for i in range(2)], axis=0
    )


def set_positions(slots, kpos):
    rows = lax.broadcasted_iota(jnp.int32, (KB, HD), 0)
    lanes = lax.broadcasted_iota(jnp.int32, (KB, HD), 1) % QB
    for e, (c, _, _, _) in enumerate(slots):
        kpos[e * KB : (e + 1) * KB] = c * KB + rows - lanes


def prob_of(sel, pair, lse, kpos, start, b, p):
    scores = lax.dot_general(sel[...], pair, NT, preferred_element_type=F32) * SCALE
    turned = pltpu.roll(lse[...], QB, 1)
    left, right = (turned, lse[...]) if b else (lse[...], turned)
    first = lax.broadcasted_iota(jnp.int32, (1, HD), 1) < QB
    row = jnp.where(first, left[2 * p : 2 * p + 1], right[2 * p + 1 : 2 * p + 2])
    return jnp.where(kpos[...] <= start, jnp.exp(scores - row), 0.0)


def scatter(slots, parts, total, send, own_sum, peers, kblocks):
    def put(slot):
        _, remote, place, within = slot
        return jnp.where(remote, place, peers + within)

    zero = jnp.zeros((KB, HD), F32)
    for k in range(kblocks):
        total[peers + k] = zero
    for slot in slots[1]:
        total[put(slot)] = zero
    for b, part in enumerate(parts):
        for e, slot in enumerate(slots[b]):
            piece = part[e * KB : (e + 1) * KB]
            at = put(slot)
            total[at] = total[at] + piece if b else piece
    for b in range(len(parts)):
        for _, remote, place, _ in slots[b]:

            @pl.when(remote)
            def _(place=place):
                send[place] = total[place].astype(BF16)

    for k in range(kblocks):
        own_sum[k] = total[peers + k]


def value_terms(nq, nz, chosen, here, queries, dout, lse, got_k, own_k, target, own_sum, sel, kpos, low, rows, total, part, send, sems):
    peers, kblocks = nq * nz, own_k.shape[0]
    qblocks, pairs = queries.shape[0] // QB, queries.shape[1] // HD // 2
    slots = [slots_of(chosen, here[0], b, nq, nz, kblocks, lambda q: q) for b in range(qblocks)]
    for b in range(qblocks):
        select(slots[b], got_k, own_k, sel)
        set_positions(slots[b], kpos)
        start = here[0] * queries.shape[0] + b * QB
        for p in range(pairs):
            pair = heads_of(queries, b, p)
            prob = prob_of(sel, pair, lse, kpos, start, b, p)
            low[:, p * HD : (p + 1) * HD] = prob.astype(BF16)
            rows[p * HD : (p + 1) * HD] = heads_of(dout, b, p)
        part[b] = jnp.dot(low[...], rows[...], preferred_element_type=F32)
    scatter(slots, [part.at[b] for b in range(qblocks)], total, send, own_sum, peers, kblocks)
    for copy in moves([(send, target)], sems):
        copy.wait()


def key_terms(nx, nc, nz, chosen, here, lse, own_k, own_v, *refs):
    nq = nx * nc
    ins, refs = refs[: 3 + nx], refs[3 + nx :]
    targets, refs = refs[:nx], refs[nx:]
    own_sum, low, sel, sel_v, kpos, rows, total, part, send, held, queries, dout, got_k, sems = refs
    got_v = tuple(held.at[s] for s in range(nx))
    copies = moves(list(zip(ins, (queries, got_k, dout, *got_v))), sems)
    for copy in copies[:2]:
        copy.wait()
    peers, kblocks = nq * nz, own_k.shape[0]
    qblocks, pairs = queries.shape[0] // QB, queries.shape[1] // HD // 2
    mine = here[0] % nq

    def behind(q):
        return (mine // nc - q // nc) % nx * nc + (mine + q) % nc

    def ahead(q):
        return (q // nc - mine // nc) % nx * nc + (mine + q) % nc

    def slots(b, where):
        return slots_of(chosen, here[0], b, nq, nz, kblocks, where)

    for b in range(qblocks):
        select(slots(b, lambda q: q), got_k, own_k, sel.at[b])
        if not b:
            for copy in copies[2:]:
                copy.wait()
        select(slots(b, behind), got_v, own_v, sel_v)
        set_positions(slots(b, ahead), kpos)
        start = here[0] * queries.shape[0] + b * QB
        for p in range(pairs):
            pair = heads_of(queries, b, p)
            prob = prob_of(sel.at[b], pair, lse, kpos, start, b, p)
            dprob = lax.dot_general(sel_v[...], heads_of(dout, b, p), NT, preferred_element_type=F32)
            delta = jnp.sum(prob * dprob, axis=0, keepdims=True)
            low[b, :, p * HD : (p + 1) * HD] = (prob * (dprob - delta)).astype(BF16)
            rows[p * HD : (p + 1) * HD] = pair
        part[b] = jnp.dot(low[b], rows[...], preferred_element_type=F32) * SCALE
    back = [slots(b, ahead) for b in range(qblocks)]
    scatter(back, [part.at[b] for b in range(qblocks)], total, send, own_sum, peers, kblocks)
    size = nc * nz
    ends = [(send.at[s * size : (s + 1) * size], to) for s, to in enumerate(targets)]
    for copy in moves(ends, sems):
        copy.wait()


def query_terms(low, sel, out):
    for b in range(low.shape[0]):
        for p in range(low.shape[2] // HD):
            got = lax.dot_general(
                low[b, :, p * HD : (p + 1) * HD], sel[b], TN, preferred_element_type=F32
            )
            for i in range(2):
                out[b * QB : (b + 1) * QB, (2 * p + i) * HD : (2 * p + i + 1) * HD] = (
                    got[i * QB : (i + 1) * QB] * SCALE
                )


def gather_home(nq, nz, asked, came, dense, total):
    blocks = dense.shape[0]
    kblocks = blocks // nz
    total[...] = jnp.zeros_like(total)
    for q in range(nq):
        for z in range(nz):
            a = asked[q, z]
            at = jnp.where(a > 0, z * kblocks + a - 1, blocks)
            total[at] = total[at] + came[q * nz + z].astype(F32)
    dense[...] = total[0:blocks].astype(BF16)


def gather_both(nc, nz, asked, here, *refs):
    *sent, dense, target, total, came, other, sems = refs
    copies = moves([(a, came.at[s]) for s, a in enumerate(sent)], sems)
    blocks = dense.shape[0]
    kblocks = blocks // nz
    total[...] = jnp.zeros_like(total)
    for s, copy in enumerate(copies):
        copy.wait()
        part = came.at[s]
        peer = across(here[0], -s, len(sent), nc)
        for i in range(2 * nz):
            a = asked[peer, i]
            at = jnp.where(a > 0, i * kblocks + a - 1, 2 * blocks)
            total[at] = total[at] + part[i].astype(F32)
    other[...] = total[blocks : 2 * blocks].astype(BF16)
    copies = moves([(other, target)], sems)
    dense[...] = total[0:blocks]
    for copy in copies:
        copy.wait()


def weight_terms(rows_out, low, dense, other, *refs):
    *features, order, out = refs
    nq, nz, tok = low.shape[0], dense.shape[0], dense.shape[1]
    mine = nz // (2 * len(features))
    feats = mine * rows_out
    for k, block in enumerate(f.at[i] for f in features for i in range(2)):
        total = jnp.dot(block[0, 0:feats], low[0], preferred_element_type=F32)
        for q in range(1, nq):
            total = total + jnp.dot(block[q, 0:feats], low[q], preferred_element_type=F32)
        total = total.astype(BF16)
        for a in range(mine):
            out[order[k] * mine + a, tok:] = total[a * rows_out : (a + 1) * rows_out]
    out[:, 0:tok] = (dense[...] + other[...].astype(F32)).astype(BF16)


def local(queries, keys, values, logsum, out_grad, normed_input, chosen):
    nz = lax.axis_size("z")
    nq = lax.axis_size(XC)
    tp = lax.axis_size("tp")
    here = lax.axis_index(KV)
    tok, cols = queries.shape
    kblocks = tok // KB
    qblocks = tok // QB
    heads = cols // HD
    span = NSEL * KB
    peers = nq * nz
    shape = jax.ShapeDtypeStruct

    names = chosen
    me = here.reshape(1).astype(jnp.int32)

    rows_out = normed_input.shape[1] * tp // peers
    mine = nz // tp
    feats = mine * rows_out
    split = call(
        functools.partial(by_feature, nq, nz, rows_out),
        shape((nq, feats + SUB, tok), BF16),
        "ssv",
    )(names, me, normed_input)
    split = to_peers(split, XC)
    asked = split[:, feats, : 2 * nz].astype(jnp.int32)
    pairs = [(i, i ^ 1) for i in range(tp)]
    cross = [(i, (i + 1 if i % 2 else i - 1) % tp) for i in range(tp)]
    my_t = lax.axis_index("tp")
    near = lax.ppermute(split, "tp", pairs)
    held = jnp.stack([split, near])
    names_of = jnp.stack([my_t, my_t ^ 1])
    planes, order = [held], [names_of]
    if tp > 2:
        planes.append(lax.ppermute(held, "tp", cross))
        over = jnp.where(my_t % 2 == 1, my_t + 1, my_t - 1 + tp) % tp
        order.append(jnp.stack([over, over ^ 1]))
    order = jnp.concatenate(order).astype(jnp.int32)
    nx, nc = lax.axis_size("x"), lax.axis_size("c")

    def around(pieces):
        turns = [[(x, (x + s) % nx) for x in range(nx)] for s in range(nx)]
        return [pieces[0]] + [lax.ppermute(pieces[s], "x", turns[s]) for s in range(1, nx)]

    def swapped(rows):
        return lax.ppermute(rows, "c", [(0, 1), (1, 0)])

    def column(rows):
        return lax.all_gather(rows, "z", axis=0, tiled=True).reshape(nz * kblocks, KB, HD)

    column_k = column(keys)
    sent = call(
        functools.partial(pick, nq, nz),
        shape((peers, KB, HD), BF16),
        "sv",
        [pltpu.VMEM((peers, KB, HD), BF16), dma(nq)],
        to="h",
    )(asked, column_k)
    got_k = to_peers(sent.reshape(nq, nz * KB, HD), XC).reshape(peers, KB, HD)
    column_v = column(values)
    other_v = swapped(column_v)
    slab = shape((nc * nz, KB, HD), BF16)
    sent = call(
        functools.partial(pick_apart, nc, nz),
        (slab,) * nx,
        "ssvv",
        [pltpu.VMEM((nx, nc * nz, KB, HD), BF16), dma(nx)],
        to="h" * nx,
    )(asked, me, column_v, other_v)
    got_v = around(sent)

    own_k = keys.reshape(kblocks, KB, HD)
    own_v = values.reshape(kblocks, KB, HD)
    lse = logsum.T
    terms = (shape((peers, KB, HD), BF16), shape((kblocks, KB, HD), F32))
    slots = pltpu.VMEM((peers, KB, HD), BF16)
    rows = pltpu.VMEM((tok, cols), BF16)
    work = [
        pltpu.VMEM((span, HD), jnp.int32),
        pltpu.VMEM((heads * QB, HD), BF16),
        pltpu.VMEM((peers + kblocks, KB, HD), F32),
        pltpu.VMEM((qblocks, span, HD), F32),
    ]

    sent_v, mine_v = call(
        functools.partial(value_terms, nq, nz),
        terms,
        "ssvvvvv",
        [pltpu.VMEM((span, HD), BF16), work[0], pltpu.VMEM((span, heads * QB), BF16), *work[1:], slots, dma(1)],
        mib=8,
        to="hv",
    )(names, me, queries, out_grad, lse, got_k, own_k)
    came_v = to_peers(sent_v.reshape(nq, nz * KB, HD), XC).reshape(peers, KB, HD)
    dense_v = call(
        functools.partial(gather_home, nq, nz),
        shape((nz * kblocks, KB, HD), BF16),
        "sv",
        [pltpu.VMEM((nz * kblocks + 1, KB, HD), F32)],
        6,
    )(asked, came_v).reshape(nz, tok, HD)
    sums_v = to_peers(dense_v, "z")
    value_grad = mine_v.reshape(tok, HD) + jnp.sum(sums_v.astype(F32), axis=0)

    *sent_k, mine_k, low, sel = call(
        functools.partial(key_terms, nx, nc, nz),
        (
            *(slab,) * nx,
            terms[1],
            shape((qblocks, span, heads * QB), BF16),
            shape((qblocks, span, HD), BF16),
        ),
        "ssvvv" + "h" * (3 + nx),
        [
            *(pltpu.VMEM((span, HD), BF16), *work, slots),
            *(pltpu.VMEM((nx, nc * nz, KB, HD), BF16), rows, rows, slots, dma(3 + nx)),
        ],
        to="h" * nx + "vvv",
    )(names, me, lse, own_k, own_v, queries, got_k, out_grad, *got_v)
    came_k = around(sent_k)
    blocks = (nz * kblocks, KB, HD)
    dense_k, other_k = call(
        functools.partial(gather_both, nc, nz),
        (shape(blocks, F32), shape(blocks, BF16)),
        "ss" + "h" * nx,
        [
            pltpu.VMEM((2 * nz * kblocks + 1, KB, HD), F32),
            pltpu.VMEM((nx, nc * nz, KB, HD), BF16),
            pltpu.VMEM(blocks, BF16),
            dma(nx),
        ],
        to="vh",
    )(asked, me, *came_k)
    other_k = swapped(other_k)
    query_grad = call(query_terms, shape((tok, cols), F32), "vv")(low, sel)

    all_low = lax.all_gather(value_grad.astype(BF16), XC, axis=0)
    both = call(
        functools.partial(weight_terms, rows_out),
        shape((nz, tok + rows_out, HD), BF16),
        "v" * (3 + len(planes)) + "s",
        mib=6,
    )(
        all_low, dense_k.reshape(nz, tok, HD), other_k.reshape(nz, tok, HD), *planes, order
    )
    both = jnp.sum(to_peers(both, "z").astype(F32), axis=0)
    key_grad = mine_k.reshape(tok, HD) + both[:tok]
    return (query_grad, key_grad, value_grad, both[tok:])


def solution(mesh):
    kv, tp = mesh.shape["kv"], mesh.shape["tp"]
    split = Mesh(mesh.devices.reshape(kv // 8, 4, 2, tp), ("z", "x", "c", "tp"))
    cut = P(KV, "tp")

    return jax.shard_map(
        local,
        mesh=split,
        in_specs=(cut, cut, cut, cut, cut, cut, P(KV, None)),
        out_specs=(cut, cut, cut, cut),
        check_vma=False,
    )
```
